32 devices in a mesh: gr: 2 (over x), fs: 8 (over z, y), tp: 2 (over core).
Axes of the slice: x: 2, y: 2, z: 4, core: 2. Of those that a mesh axis runs over, the one named last changes fastest.
Arguments:
- tokens: bfloat16 [2816, 2048], P(('gr', 'fs')), may hold values from -6 to 6
- expert_ids: int32 [2816, 8], P(('gr', 'fs')), may hold values from 0 to 15, all different within a row; in each aligned block of 176 rows (0 to 175, 176 to 351, ...) at most 110 rows name the same one
- route_weight: float32 [2816, 8], P(('gr', 'fs')), may hold values from 0.05 to 1
- norm_gain: float32 [2048], P('tp'), may hold values from 0.1 to 1.9
- expert_gate: float32 [16, 512, 2048], P('gr', 'fs', 'tp'), may hold values from -0.125 to 0.125
- expert_up: float32 [16, 512, 2048], P('gr', 'fs', 'tp'), may hold values from -0.125 to 0.125
- expert_down: float32 [16, 512, 2048], P('gr', 'fs', 'tp'), may hold values from -0.25 to 0.25
- shared_gate: float32 [512, 2048], P('fs', 'tp'), may hold values from -0.125 to 0.125
- shared_up: float32 [512, 2048], P('fs', 'tp'), may hold values from -0.125 to 0.125
- shared_down: float32 [512, 2048], P('fs', 'tp'), may hold values from -0.25 to 0.25
Outputs:
- mixed: bfloat16 [2816, 2048], P(('gr', 'fs'), 'tp')
- new_gate: bfloat16 [2, 8, 512, 2048], P(None, 'fs', None, 'tp')
- new_up: bfloat16 [2, 8, 512, 2048], P(None, 'fs', None, 'tp')
- new_down: bfloat16 [2, 8, 512, 2048], P(None, 'fs', None, 'tp')
- new_shared_gate: bfloat16 [512, 2048], P(None, 'tp')
- new_shared_up: bfloat16 [512, 2048], P(None, 'tp')
- new_shared_down: bfloat16 [512, 2048], P(None, 'tp')
The draws below stay inside these ranges and needn't reach their ends.
Inputs may be any that keep to these rules, and one draw needn't show every extreme that they name: `expert_ids`: each row names 8 different experts; within each aligned block of 176 rows no expert is named by more than 110 rows, a bound that some block reaches.
All inputs are finite; a program needn't handle non-finite values.
Results may differ from the reference program's by a relative error of at most 0.022.
Values may be sent and summed in bfloat16 or wider, within the bound.
A program may use at most 128 MiB of HBM per device.

```python
import math
import jax
import jax.numpy as jnp
import numpy as np
from jax import lax

D = 2048
FF = 512
SHARED = 512
TOP = 8
TOK_DEV = 176
EXPERTS = 16
CAP = 110
TOKENS = 2816
N_GR = 2
N_FS = 8
N_TP = 2


def shard_levels(key, extent, shards, low, high):
    factor_of, own = 1.0, jax.random.fold_in(key, 6)
    for position, shards_of in shards:
        heights = jnp.exp(jax.random.uniform(jax.random.fold_in(own, position), (shards_of,), jnp.float32, low / len(shards), high / len(shards)))
        factor_of = factor_of * jnp.repeat(heights, extent[position] // shards_of).reshape([-1 if axis == position else 1 for axis in range(len(extent))])
    return factor_of


def routed_block(stream_key, own, number, rows, amount, top, limit, slope):
    sequence = jax.random.permutation(stream_key, amount)
    crowded, common = shares(amount, rows * top, limit, slope, True), shares(amount, rows * top, limit, slope, False)
    places = jnp.arange(amount)

    def named(tallies, offset_by):
        used = int((tallies > 0).sum())
        fixed = max(1, used // 4)
        moved = fixed + (places - fixed + offset_by * (used - fixed)) % max(1, amount - fixed)
        return jnp.zeros((amount,), jnp.int32).at[sequence[jnp.where(places < fixed, places, moved)]].set(jnp.asarray(tallies, jnp.int32))

    tallies = jnp.where(number % 4 == 0, named(crowded, number // 4), named(common, number - number // 4 - 1))
    mixed = jax.random.permutation(jax.random.fold_in(own, 3), amount)
    giver, taker = mixed[0:amount // 2 * 2:2], mixed[1:amount // 2 * 2:2]
    slack = jnp.minimum(tallies[giver] - 1, limit - tallies[taker]) // 2
    slack = jnp.where((giver == sequence[0]) | (taker == sequence[0]) | (tallies[taker] == 0), 0, jnp.maximum(slack, 0))
    moved = jax.random.randint(jax.random.fold_in(own, 4), (amount // 2,), 0, 1 << 20) % (slack + 1)
    tallies = tallies.at[giver].add(-moved).at[taker].add(moved)
    labels = jnp.searchsorted(jnp.cumsum(tallies), jnp.arange(rows * top), side="right").astype(jnp.int32)
    listing = labels.reshape(top, rows).T
    listing = listing[jax.random.permutation(jax.random.fold_in(own, 1), rows)]
    offset_by = jax.random.randint(jax.random.fold_in(own, 2), (rows, 1), 0, top)
    return jnp.take_along_axis(listing, (jnp.arange(top)[None, :] + offset_by) % top, axis=1)


def shares(count, total, bound, slope, full):
    loads = [(1 << 20) // math.isqrt(grade ** slope) + 1 for grade in range(1, count + 1)]
    largest = bound if full else min(bound, max(-(-total // count), total * loads[0] // sum(loads)))
    least = 1 if total - largest >= count - 1 else 0
    counts, surplus = [largest] + [least] * (count - 1), total - largest - least * (count - 1)
    while surplus > 0:
        candidates = [i for i in range(1, count) if counts[i] < largest] or [i for i in range(1, count) if counts[i] < bound]
        whole, left = sum([loads[i] for i in candidates]), surplus
        for i in candidates:
            more = min(bound - counts[i], max(1, left * loads[i] // whole), surplus)
            counts[i] = counts[i] + more
            surplus = surplus - more
    return np.array(counts)


def centred(own_key, dims, spread, reach, pieces=(), kind=jnp.bfloat16):
    entries = spread * jax.random.normal(own_key, dims, jnp.float32)
    if pieces:
        entries = entries * shard_levels(own_key, dims, pieces, -0.22, 0.18)
    return jnp.clip(entries, -reach, reach).astype(kind)


def setup_inputs(seed: int = 0) -> dict:
    splits = jax.random.split(jax.random.key(seed), 11)
    tokens = centred(splits[0], (TOKENS, D), 1.0, 6.0, ((0, 16),))
    expert_ids_keys = jax.random.split(jax.random.fold_in(splits[1], 1), TOKENS // TOK_DEV)
    expert_ids_turns = jax.random.permutation(jax.random.fold_in(splits[1], 3), TOKENS // TOK_DEV)
    expert_ids = jax.vmap(lambda own, number: routed_block(jax.random.fold_in(splits[1], 2), own, number, TOK_DEV, EXPERTS, TOP, CAP, 1))(expert_ids_keys, expert_ids_turns).reshape((TOKENS, TOP))
    route_weight = jnp.clip(jnp.exp(math.log(1.0) - 2.9957323 * jax.random.uniform(splits[2], (TOKENS, TOP), jnp.float32) ** shard_levels(splits[2], (TOKENS, TOP), ((0, 16),), -0.2, 0.2)), 0.05, 1.0)
    norm_gain = jnp.clip(1.0 + 0.18 * jax.random.normal(splits[3], (D,), jnp.float32), 0.1, 1.9)
    expert_gate = centred(splits[4], (EXPERTS, FF, D), D ** -0.5, 0.125, ((0, 2), (1, 8), (2, 2)), jnp.float32)
    expert_up = centred(splits[5], (EXPERTS, FF, D), D ** -0.5, 0.125, ((0, 2), (1, 8), (2, 2)), jnp.float32)
    expert_down = centred(splits[6], (EXPERTS, FF, D), FF ** -0.5, 0.25, ((0, 2), (1, 8), (2, 2)), jnp.float32)
    shared_gate = centred(splits[7], (SHARED, D), D ** -0.5, 0.125, ((0, 8), (1, 2)), jnp.float32)
    shared_up = centred(splits[8], (SHARED, D), D ** -0.5, 0.125, ((0, 8), (1, 2)), jnp.float32)
    shared_down = centred(splits[9], (SHARED, D), SHARED ** -0.5, 0.25, ((0, 8), (1, 2)), jnp.float32)
    return dict(tokens=tokens, expert_ids=expert_ids, route_weight=route_weight, norm_gain=norm_gain, expert_gate=expert_gate, expert_up=expert_up, expert_down=expert_down, shared_gate=shared_gate, shared_up=shared_up, shared_down=shared_down)


route_scale = 2.5
norm_eps = 1e-06

def blocked_product(rows, weight):
    count = rows.shape[0]
    left = rows.astype(jnp.float32).reshape(count, N_TP, D // N_TP)
    right = weight.astype(jnp.float32).reshape(weight.shape[0], N_TP, D // N_TP)
    parts = jnp.einsum('mbd,fbd->bmf', left, right, precision=lax.Precision.HIGHEST).astype(jnp.bfloat16)
    parts = lax.optimization_barrier(parts)
    return lax.optimization_barrier(jnp.sum(parts.astype(jnp.float32), axis=0))

def feed_forward(rows, gate_weight, up_weight):
    gate_pre = blocked_product(rows, gate_weight)
    up_pre = blocked_product(rows, up_weight)
    return (jax.nn.silu(gate_pre) * up_pre).astype(jnp.bfloat16)

def reference(tokens, expert_ids, route_weight, norm_gain, expert_gate, expert_up, expert_down, shared_gate, shared_up, shared_down):
    gate_round = (expert_gate * norm_gain).astype(jnp.bfloat16)
    up_round = (expert_up * norm_gain).astype(jnp.bfloat16)
    down_round = expert_down.astype(jnp.bfloat16)
    shared_gate_round = (shared_gate * norm_gain).astype(jnp.bfloat16)
    shared_up_round = (shared_up * norm_gain).astype(jnp.bfloat16)
    shared_down_round = shared_down.astype(jnp.bfloat16)
    tok_float = tokens.astype(jnp.float32)
    normed = (tok_float * lax.rsqrt(lax.optimization_barrier(jnp.mean(tok_float * tok_float, axis=1, keepdims=True)) + norm_eps)).astype(jnp.bfloat16)
    share = route_weight / lax.optimization_barrier(jnp.sum(route_weight, axis=1, keepdims=True)) * route_scale
    shared_act = feed_forward(normed, shared_gate_round, shared_up_round)
    shared_out = jnp.dot(shared_act, shared_down_round, preferred_element_type=jnp.float32)
    most_rows = EXPERTS * CAP

    def per_expert(total, expert):
        named = expert_ids == expert
        chosen = lax.optimization_barrier(jnp.sum(jnp.where(named, share, jnp.float32(0.0)), axis=1))
        present = jnp.any(named, axis=1)
        index = jnp.nonzero(present, size=most_rows, fill_value=0)[0].astype(jnp.int32)
        live = jnp.arange(most_rows).astype(jnp.int32) < jnp.sum(present.astype(jnp.int32))
        picked = normed[index]
        act = feed_forward(picked, gate_round[expert], up_round[expert])
        out = jnp.dot(act, down_round[expert], preferred_element_type=jnp.float32).astype(jnp.bfloat16)
        scale = jnp.where(live, chosen[index], jnp.float32(0.0))
        return (total.at[index].add(scale[:, None] * out.astype(jnp.float32)), None)
    start_total = jnp.zeros((TOKENS, D), jnp.float32)
    routed, _ = lax.scan(per_expert, start_total, jnp.arange(EXPERTS).astype(jnp.int32))
    mixed = (shared_out + routed).astype(jnp.bfloat16)
    new_gate = gate_round.reshape(N_GR, N_FS, FF, D)
    new_up = up_round.reshape(N_GR, N_FS, FF, D)
    new_down = down_round.reshape(N_GR, N_FS, FF, D)
    return (mixed, new_gate, new_up, new_down, shared_gate_round, shared_up_round, shared_down_round)
```

```python
import functools

import jax
import jax.numpy as jnp
from jax import lax
from jax.experimental import pallas as pl
from jax.experimental.pallas import tpu as pltpu
from jax.sharding import PartitionSpec as P

route_scale = 2.5
norm_eps = 1e-06
vmem_bytes = 67043328


def fold_gain(weight, gain):
    return (weight * gain).astype(jnp.bfloat16)


def silu(v):
    return v / (1.0 + jnp.exp(-v))


def handover(
    dims,
    tok,
    w0,
    w1,
    w2,
    s0,
    s1,
    s2,
    mixed,
    n0,
    n1,
    n2,
    h0,
    h1,
    h2,
    xs,
    pout,
    pin,
    act,
    oz,
    rety,
    ret,
    psh,
    pshin,
    local_sem,
    tok_send,
    tok_recv,
    w_send,
    w_recv,
    x_send,
    x_recv,
    sh_send,
    sh_recv,
    shx_send,
    shx_recv,
    p_send,
    p_recv,
    a_send,
    a_recv,
    ry_send,
    ry_recv,
    r_send,
    r_recv,
    ps_send,
    ps_recv,
):
    G, S, TP, T, C, H, F, SF, slots, Y = dims
    Z = S // Y
    E = G * S
    SH = SF * S
    NB = S // TP
    NH = NB * T
    gi, si, ti = lax.axis_index("gr"), lax.axis_index("fs"), lax.axis_index("tp")
    zi, yi = si // Y, lax.rem(si, Y)
    w, new, sh, shn = (w0, w1, w2), (n0, n1, n2), (s0, s1, s2), (h0, h1, h2)

    def rdma(src, dst, ssem, rsem, dev):
        return pltpu.make_async_remote_copy(
            src_ref=src,
            dst_ref=dst,
            send_sem=ssem,
            recv_sem=rsem,
            device_id=dev,
            device_id_type=pl.DeviceIdType.MESH,
        )

    def rows(start, step, size):
        return pl.ds(pl.multiple_of(start * step, step), size)

    def each(lo, hi, fn):
        def step(i, c):
            fn(i)
            return c

        lax.fori_loop(lo, hi, step, 0)

    def fs_peer(k):
        return lax.rem(si + k, S)

    def fs_from(k):
        return lax.rem(si + S - k, S)

    def gr_peer(k):
        return lax.rem(gi + k, G)

    def tp_peer(k):
        return lax.rem(ti + k, TP)

    barrier = pltpu.get_barrier_semaphore()

    def greet(axis, peer, n):
        each(
            1,
            n,
            lambda k: pl.semaphore_signal(
                barrier,
                inc=1,
                device_id={axis: peer(k)},
                device_id_type=pl.DeviceIdType.MESH,
            ),
        )

    greet("fs", fs_peer, S)
    greet("gr", gr_peer, G)
    greet("tp", tp_peer, TP)
    pl.semaphore_wait(barrier, S + G + TP - 3)

    def w_copy(m, d, s):
        return rdma(
            w[m].at[d], new[m].at[gi, rows(s, F, F)], w_send.at[m, d], w_recv.at[m, s], {"fs": d}
        )

    def spread(block, s, up, down, act_on, own=False):
        src, place, ssem, rsem, after = block
        at = place(s)

        def hop(way, dev):
            act_on(rdma(src if own else at, at, ssem.at[s, way], rsem.at[s], {"fs": dev}))

        if up:
            pl.when(zi < Z - 1)(lambda: hop(0, si + Y))
        if down:
            pl.when(zi > 0)(lambda: hop(1, si - Y))

        def across(k):
            y = lax.rem(yi + k, Y)
            hop(2 + y, zi * Y + y)

        each(1, Y, across)

    def shx_copy(m, s, g, dev):
        at = sh_place(m, s, g)
        return rdma(at, at, shx_send.at[m, s, dev], shx_recv.at[m, s, g], {"gr": dev})

    def arrive(block, s):
        src, place, ssem, rsem, after = block
        rdma(place(s), place(s), ssem.at[s, 0], rsem.at[s], {"fs": fs_peer(1)}).wait_recv()
        if after is not None:
            after(s)

    def start(c):
        c.start()

    def sent(c):
        c.wait_send()

    def relay(block, step, act_on=start):
        def from_below():
            s = si - step * Y
            if act_on is start:
                arrive(block, s)
            spread(block, s, True, False, act_on)

        def from_above():
            s = si + step * Y
            if act_on is start:
                arrive(block, s)
            spread(block, s, False, True, act_on)

        pl.when(zi >= step)(from_below)
        pl.when(zi + step < Z)(from_above)

    def others_arrive(block, step):
        def at(z):
            each(1, Y, lambda k: arrive(block, z * Y + lax.rem(yi + k, Y)))

        if step == 0:
            at(zi)
        else:
            pl.when(zi >= step)(lambda: at(zi - step))
            pl.when(zi + step < Z)(lambda: at(zi + step))

    def block_sent(block):
        spread(block, si, True, True, sent, own=True)
        for step in range(1, Z):
            relay(block, step, sent)

    def sh_place(m, s, g):
        return shn[m].at[rows(s, SF, SF), rows(g, C // G, C // G)]

    def sh_block(m):
        return (
            sh[m].at[:, rows(gi, C // G, C // G)],
            lambda s: sh_place(m, s, gi),
            sh_send.at[m],
            sh_recv.at[m],
            lambda s: each(1, G, lambda j: shx_copy(m, s, gi, gr_peer(j)).start()),
        )

    tok_block = (tok, lambda s: xs.at[rows(s, T, T)], tok_send, tok_recv, None)
    sh_blocks = [sh_block(m) for m in range(3)]

    def shared_step(step):
        for block in sh_blocks:
            if step < Z:
                relay(block, step)
            others_arrive(block, step - 1)

    def x_copy(m, s, g, dev, own=False):
        place = new[m].at[g, rows(s, F, F)]
        src = w[m].at[s] if own else place
        return rdma(src, place, x_send.at[m, s, dev], x_recv.at[m, s, g], {"gr": dev})

    def local_copies():
        return (
            [pltpu.make_async_copy(w[m].at[si], new[m].at[gi, rows(si, F, F)], local_sem.at[m]) for m in range(3)]
            + [pltpu.make_async_copy(sh[m], shn[m].at[rows(si, SF, SF)], local_sem.at[3 + m]) for m in range(3)]
            + [pltpu.make_async_copy(tok, xs.at[rows(si, T, T)], local_sem.at[6])]
        )

    def send_weight(m):
        each(1, S, lambda k: w_copy(m, fs_peer(k), si).start())

    for m in range(3):
        each(1, G, lambda j, m=m: x_copy(m, si, gi, gr_peer(j), own=True).start())
    spread(tok_block, si, True, True, start, own=True)
    send_weight(0)
    for copy in local_copies():
        copy.start()

    def forward(m, lo=1, hi=S):
        def one(k):
            s = fs_from(k)
            w_copy(m, s, s).wait_recv()
            each(1, G, lambda j: x_copy(m, s, gi, gr_peer(j)).start())

        each(lo, hi, one)

    def x_arrive(m, g):
        each(0, S, lambda s: x_copy(m, s, g, g).wait_recv())

    def p_copy(j, t, s):
        return rdma(
            pout.at[j if slots > 1 else 0, t], pin.at[j, s], p_send.at[j, t], p_recv.at[j, s], {"tp": t}
        )

    def a_copy(j, t, s):
        place = act.at[j, rows(s, NH, NH)]
        return rdma(place, place, a_send.at[j, t], a_recv.at[j, s], {"tp": t})

    def first_matmuls(j):
        g = gr_peer(j)
        slot = j if slots > 1 else 0
        for q in range(TP):
            t = tp_peer(1 + q)

            def block(b, t=t):
                x = xs[rows(t * NB + b, T, T), 0:C]
                for m in range(2):
                    part = lax.dot_general(
                        x, new[m][g], (((1,), (1,)), ((), ())), preferred_element_type=jnp.float32
                    )
                    pout[slot, t, rows(b, T, T), m * H : (m + 1) * H] = part.astype(jnp.bfloat16)

            each(0, NB, block)
            if q < TP - 1:
                p_copy(j, t, ti).start()

    def activations(j):
        g = gr_peer(j)
        slot = j if slots > 1 else 0
        expert = g * S + si
        for q in range(1, TP):
            t = tp_peer(q)
            p_copy(j, t, t).wait_recv()

        def block(b):
            r = rows(b, T, T)
            pre = pout[slot, ti, r, :].astype(jnp.float32)
            for q in range(1, TP):
                pre = pre + pin[j, tp_peer(q), r, :].astype(jnp.float32)
            at = rows(ti * NB + b, T, T)
            coded = xs[at, C:].astype(jnp.float32)
            lane = lax.broadcasted_iota(jnp.int32, coded.shape, 1)
            share = jnp.sum(
                jnp.where((lane == expert) | (lane == expert + E), coded, 0.0), axis=1, keepdims=True
            )
            value = silu(pre[:, :H]) * pre[:, H:] * share
            act[j, at, :] = value.astype(jnp.bfloat16)

        each(0, NB, block)
        for q in range(1, TP):
            a_copy(j, tp_peer(q), ti).start()

    if Z > 1:
        relay(tok_block, 1)
    send_weight(1)
    forward(0)
    for step in range(2, Z):
        relay(tok_block, step)
    send_weight(2)
    for block in sh_blocks:
        spread(block, si, True, True, start, own=True)
    forward(1)
    for copy in local_copies():
        copy.wait()
    for step in range(Z):
        others_arrive(tok_block, step)
    for j in range(G):
        if j > 0:
            for m in range(2):
                x_arrive(m, gr_peer(j))
            if slots == 1:
                for q in range(1, TP):
                    p_copy(j - 1, tp_peer(q), ti).wait_send()
        first_matmuls(j)
        if j == 1:
            forward(2, S // 2, S)
        activations(j)
        if j == 0:
            forward(2, 1, S // 2 if G > 1 else S)
    shared_step(1)

    for j in range(1, G):
        x_arrive(2, gr_peer(j))

    def ry_copy(z, y, src):
        return rdma(
            oz.at[rows(z * Y + y, T, T)],
            rety.at[z, src],
            ry_send.at[z, y],
            ry_recv.at[z, src],
            {"fs": zi * Y + y},
        )

    def r_copy(z, up, dist):
        slot = Z if dist == 1 and not up else z
        return rdma(
            oz.at[rows(z * Y + yi, T, T)],
            ret.at[slot],
            r_send.at[z],
            r_recv.at[slot],
            {"fs": si + Y if up else si - Y},
        )

    def far_first(fn):
        for dist in range(Z - 1, -1, -1):
            pl.when(zi + dist < Z)(functools.partial(fn, zi + dist, True, dist))
            if dist:
                pl.when(zi >= dist)(functools.partial(fn, zi - dist, False, dist))

    for q in range(1, TP):
        for j in range(G):
            a_copy(j, tp_peer(q), tp_peer(q)).wait_recv()

    def down_block(z, up, dist):
        def column(k):
            y = lax.rem(yi + k, Y)
            at = rows(z * Y + y, T, T)
            total = jnp.zeros((T, C), jnp.float32)
            for j in range(G):
                total = total + jnp.dot(
                    act[j, at, :], new[2][gr_peer(j)], preferred_element_type=jnp.float32
                )
            oz[at, :] = total.astype(jnp.bfloat16)
            pl.when(y != yi)(lambda: ry_copy(z, y, yi).start())

        each(1, Y + 1, column)

    far_first(down_block)
    if Z > 1:
        shared_step(2)

    def add_far(z, slot):
        at = rows(z * Y + yi, T, T)
        rdma(
            ret.at[slot], ret.at[slot], r_send.at[z], r_recv.at[slot], {"fs": fs_peer(1)}
        ).wait_recv()
        total = oz[at, :].astype(jnp.float32) + ret[slot].astype(jnp.float32)
        oz[at, :] = total.astype(jnp.bfloat16)

    def column_sum(z, up, dist):
        at = rows(z * Y + yi, T, T)
        total = oz[at, :].astype(jnp.float32)
        for k in range(1, Y):
            y = lax.rem(yi + k, Y)
            ry_copy(z, y, y).wait_recv()
            total = total + rety[z, y].astype(jnp.float32)
        oz[at, :] = total.astype(jnp.bfloat16)
        if dist == 0 or up:
            pl.when(zi > 0)(lambda: add_far(z, z))
        if dist == 0:
            pl.when(zi < Z - 1)(lambda: add_far(z, Z))
        elif not up:
            pl.when(zi < Z - 1)(lambda: add_far(z, z))
        if dist:
            r_copy(z, up, dist).start()

    far_first(column_sum)
    for step in range(3, Z + 1):
        shared_step(step)

    def shared_arrive(m):
        each(
            1,
            S,
            lambda k: each(
                1, G, lambda j: shx_copy(m, fs_from(k), gr_peer(j), gr_peer(j)).wait_recv()
            ),
        )

    def ps_copy(t, s):
        return rdma(psh, pshin.at[s], ps_send.at[t], ps_recv.at[s], {"tp": t})

    for m in range(2):
        shared_arrive(m)
        part = lax.dot_general(
            xs[rows(si, T, T), 0:C],
            shn[m][...],
            (((1,), (1,)), ((), ())),
            preferred_element_type=jnp.float32,
        )
        psh[:, m * SH : (m + 1) * SH] = part.astype(jnp.bfloat16)
    for q in range(1, TP):
        ps_copy(tp_peer(q), ti).start()
    shared_arrive(2)
    pre = psh[...].astype(jnp.float32)
    for q in range(1, TP):
        t = tp_peer(q)
        ps_copy(t, t).wait_recv()
        pre = pre + pshin[t].astype(jnp.float32)
    shared_act = (silu(pre[:, :SH]) * pre[:, SH:]).astype(jnp.bfloat16)
    total = jnp.dot(shared_act, shn[2][...], preferred_element_type=jnp.float32)
    total = total + oz[rows(si, T, T), :].astype(jnp.float32)
    mixed[...] = total.astype(jnp.bfloat16)

    for m in range(3):
        each(1, S, lambda k, m=m: w_copy(m, fs_peer(k), si).wait_send())
        block_sent(sh_blocks[m])
        each(
            1,
            S,
            lambda k, m=m: each(
                1, G, lambda j: shx_copy(m, fs_from(k), gi, gr_peer(j)).wait_send()
            ),
        )
        each(0, S, lambda s, m=m: each(1, G, lambda j: x_copy(m, s, gi, gr_peer(j)).wait_send()))
    block_sent(tok_block)
    each(0, Z, lambda z: each(1, Y, lambda k: ry_copy(z, lax.rem(yi + k, Y), yi).wait_send()))

    def r_sent(z, up, dist):
        if dist:
            r_copy(z, up, dist).wait_send()

    far_first(r_sent)
    for q in range(1, TP):
        t = tp_peer(q)
        ps_copy(t, ti).wait_send()
        for j in range(G):
            if slots > 1 or j == G - 1:
                p_copy(j, t, ti).wait_send()
            a_copy(j, t, ti).wait_send()


def emit_kernel(*refs):
    n = len(refs) // 2
    sem = refs[-1]
    copies = []
    for i in range(n):
        dst = refs[n + i]
        if len(dst.shape) == 4:
            dst = dst.at[:, 0]
        copies.append(pltpu.make_async_copy(refs[i], dst, sem.at[i]))
    for c in copies:
        c.start()
    for c in copies:
        c.wait()


def emit(results, G):
    bf16 = jnp.bfloat16
    shapes = [r.shape if len(r.shape) < 3 else (r.shape[0], 1) + r.shape[1:] for r in results]
    n = len(results)
    return pl.pallas_call(
        emit_kernel,
        out_shape=[jax.ShapeDtypeStruct(s, bf16) for s in shapes],
        in_specs=[pl.BlockSpec(memory_space=pltpu.VMEM)] * n,
        out_specs=[pl.BlockSpec(memory_space=pl.ANY)] * n,
        scratch_shapes=[pltpu.SemaphoreType.DMA((n,))],
        compiler_params=pltpu.CompilerParams(vmem_limit_bytes=vmem_bytes // 2),
        name="emit",
    )(*results)


def body(
    Y,
    tokens,
    expert_ids,
    route_weight,
    norm_gain,
    expert_gate,
    expert_up,
    expert_down,
    shared_gate,
    shared_up,
    shared_down,
):
    G, S, TP = lax.axis_size("gr"), lax.axis_size("fs"), lax.axis_size("tp")
    T, C = tokens.shape[0], expert_gate.shape[2]
    F, SF = expert_gate.shape[1], shared_gate.shape[0]
    H, SH = F * S, SF * S
    E, N = G * S, S * T
    NH = N // TP
    lanes = -(-2 * E // 128) * 128
    bf16 = jnp.bfloat16

    tok_float = tokens.astype(jnp.float32)
    normed = (
        tok_float * lax.rsqrt(jnp.mean(tok_float * tok_float, axis=1, keepdims=True) + norm_eps)
    ).astype(bf16)
    normed_cols = lax.dynamic_slice_in_dim(normed, lax.axis_index("tp") * C, C, 1)
    share = route_weight / jnp.sum(route_weight, axis=1, keepdims=True) * route_scale
    lane = jnp.arange(lanes, dtype=jnp.int32)[None, None, :]
    dense = jnp.sum(
        jnp.where(expert_ids[:, :, None] == lane % E, share[:, :, None], 0.0), axis=1
    )
    high = dense.astype(bf16)
    low = (dense - lax.reduce_precision(dense, 8, 7)).astype(bf16)
    place = lane[0]
    coded = jnp.where(place < E, high, jnp.where(place < 2 * E, low, 0))
    payload = jnp.concatenate([normed_cols, coded.astype(bf16)], axis=1)

    weights = (
        fold_gain(expert_gate, norm_gain),
        fold_gain(expert_up, norm_gain),
        expert_down.astype(bf16),
    )
    shared = (
        fold_gain(shared_gate, norm_gain),
        fold_gain(shared_up, norm_gain),
        shared_down.astype(bf16),
    )
    row_bytes = 2 * (2 * G * 2 * H + G * H + 3 * C + lanes)
    slots = G if N * row_bytes < vmem_bytes * 3 // 5 else 1
    dims = (G, S, TP, T, C, H, F, SF, slots, Y)
    vmem, hbm = pl.BlockSpec(memory_space=pltpu.VMEM), pl.BlockSpec(memory_space=pl.ANY)
    dma = pltpu.SemaphoreType.DMA
    out_bytes = 2 * C * (T + 3 * G * H + 3 * SH)
    results = pl.pallas_call(
        functools.partial(handover, dims),
        out_shape=[pltpu.VMEM((T, C), bf16)]
        + [pltpu.VMEM((G, H, C), bf16)] * 3
        + [pltpu.VMEM((SH, C), bf16)] * 3,
        in_specs=[vmem] * 7,
        out_specs=[vmem] * 7,
        scratch_shapes=[
            pltpu.VMEM((N, C + lanes), bf16),
            pltpu.VMEM((slots, TP, NH, 2 * H), bf16),
            pltpu.VMEM((G, TP, NH, 2 * H), bf16),
            pltpu.VMEM((G, N, H), bf16),
            pltpu.VMEM((N, C), bf16),
            pltpu.VMEM((S // Y, Y, T, C), bf16),
            pltpu.VMEM((S // Y + 1, T, C), bf16),
            pltpu.VMEM((T, 2 * SH), bf16),
            pltpu.VMEM((TP, T, 2 * SH), bf16),
            dma((7,)),
            dma((S, 2 + Y)),
            dma((S,)),
            dma((3, S)),
            dma((3, S)),
            dma((3, S, G)),
            dma((3, S, G)),
            dma((3, S, 2 + Y)),
            dma((3, S)),
            dma((3, S, G)),
            dma((3, S, G)),
            dma((G, TP)),
            dma((G, TP)),
            dma((G, TP)),
            dma((G, TP)),
            dma((S // Y, Y)),
            dma((S // Y, Y)),
            dma((S // Y,)),
            dma((S // Y + 1,)),
            dma((TP,)),
            dma((TP,)),
        ],
        compiler_params=pltpu.CompilerParams(
            collective_id=0, has_side_effects=True, vmem_limit_bytes=vmem_bytes - 5 * out_bytes // 4
        ),
        name="handover",
    )(payload, *weights, *shared)
    return emit(results, G)


def line_length(mesh):
    places = [d.coords for d in mesh.devices[0, :, 0]]
    axis = [i for i in range(3) if places[0][i] != places[1][i]][0]
    count = 0
    for place in places:
        if any(place[i] != places[0][i] for i in range(3) if i != axis):
            break
        count += 1
    return count if len(places) % count == 0 else len(places)


def solution(mesh):
    placed = (
        P(("gr", "fs"), None),
        P(("gr", "fs"), None),
        P(("gr", "fs"), None),
        P("tp"),
        P("gr", "fs", "tp"),
        P("gr", "fs", "tp"),
        P("gr", "fs", "tp"),
        P("fs", "tp"),
        P("fs", "tp"),
        P("fs", "tp"),
    )
    return jax.shard_map(
        functools.partial(body, line_length(mesh)),
        mesh=mesh,
        in_specs=placed,
        out_specs=(
            P(("gr", "fs"), "tp"),
            P(None, "fs", None, "tp"),
            P(None, "fs", None, "tp"),
            P(None, "fs", None, "tp"),
            P(None, "tp"),
            P(None, "tp"),
            P(None, "tp"),
        ),
        check_vma=False,
    )
```

```python
import functools

import jax
import jax.numpy as jnp
from jax import lax
from jax.experimental import pallas as pl
from jax.experimental.pallas import tpu as pltpu
from jax.sharding import PartitionSpec as P

SCHEDULE = ('B', 'T', 'C0', 'X0', 'W0:0:4', 'C1', 'C2', 'c', 'X1', 'X2', 'R1', 'W0:4:8', 'F0:0:4', 'R2', 'W1:0:4', 'F0:4:8', 'R3', 'W1:4:8', 'W2', 'F1', 'S', 'F2:0:4', 'O0', 'O1', 'O2', 'O3', 'M0', 'V0', 'F2:4:8', 'A0', 'A1', 's0', 'M1', 'V1', 's1', 'A2', 'a', 'D0', 's2', 's3', 'G0', 'H', 'P', 'E')
route_scale = 2.5
norm_eps = 1e-06
vmem_bytes = 67043328


def fold_gain(weight, gain):
    return (weight * gain).astype(jnp.bfloat16)


def silu(v):
    return v / (1.0 + jnp.exp(-v))


def handover(
    dims,
    tok,
    ids,
    scores,
    gain,
    w0,
    w1,
    w2,
    s0,
    s1,
    s2,
    mixed,
    n0,
    n1,
    n2,
    h0,
    h1,
    h2,
    tokv,
    wf,
    sf,
    wb,
    xs,
    pout,
    pin,
    act,
    oz,
    rety,
    ret,
    psh,
    pshin,
    in_sem,
    tok_send,
    tok_recv,
    w_send,
    w_recv,
    x_send,
    x_recv,
    sh_send,
    sh_recv,
    shx_send,
    shx_recv,
    p_send,
    p_recv,
    a_send,
    a_recv,
    ry_send,
    ry_recv,
    r_send,
    r_recv,
    ps_send,
    ps_recv,
):
    G, S, TP, T, C, H, F, SF, slots, Y, halves, modes = dims
    Z = S // Y
    E = G * S
    SH = SF * S
    NB = S // TP
    NH = NB * T
    gi, si, ti = lax.axis_index("gr"), lax.axis_index("fs"), lax.axis_index("tp")
    zi, yi = si // Y, lax.rem(si, Y)
    w, new, sh, shn = (w0, w1, w2), (n0, n1, n2), (s0, s1, s2), (h0, h1, h2)
    HW, pieces = C // halves, len(modes)
    CW = C // pieces
    parts = [(0, 0, C), (1, 0, C)] + [(2, h * HW, HW) for h in range(halves)]

    def rdma(src, dst, ssem, rsem, dev):
        return pltpu.make_async_remote_copy(
            src_ref=src,
            dst_ref=dst,
            send_sem=ssem,
            recv_sem=rsem,
            device_id=dev,
            device_id_type=pl.DeviceIdType.MESH,
        )

    def rows(start, step, size):
        return pl.ds(pl.multiple_of(start * step, step), size)

    def each(lo, hi, fn):
        def step(i, c):
            fn(i)
            return c

        lax.fori_loop(lo, hi, step, 0)

    def fs_peer(k):
        return lax.rem(si + k, S)

    def fs_from(k):
        return lax.rem(si + S - k, S)

    def gr_peer(k):
        return lax.rem(gi + k, G)

    def tp_peer(k):
        return lax.rem(ti + k, TP)

    barrier = pltpu.get_barrier_semaphore()

    def greet(axis, peer, n):
        each(
            1,
            n,
            lambda k: pl.semaphore_signal(
                barrier,
                inc=1,
                device_id={axis: peer(k)},
                device_id_type=pl.DeviceIdType.MESH,
            ),
        )

    greet("fs", fs_peer, S)
    greet("gr", gr_peer, G)
    greet("tp", tp_peer, TP)
    inputs = [
        pltpu.make_async_copy(tok, tokv, in_sem.at[0]),
        *(pltpu.make_async_copy(w[m], wf.at[m], in_sem.at[1 + m]) for m in range(3)),
        *(pltpu.make_async_copy(sh[m], sf.at[m], in_sem.at[4 + m]) for m in range(3)),
    ]
    for copy in inputs:
        copy.start()

    def route_codes():
        share = scores[...] / jnp.sum(scores[...], axis=0, keepdims=True) * route_scale
        expert = lax.broadcasted_iota(jnp.int32, (E, T), 0)
        dense = jnp.zeros((E, T), jnp.float32)
        for k in range(ids.shape[0]):
            dense = dense + jnp.where(expert == ids[k : k + 1, :], share[k : k + 1, :], 0.0)
        high = dense.astype(jnp.bfloat16).astype(jnp.float32)
        coded = [high, dense - high]
        if C + 2 * E < xs.shape[1]:
            coded.append(jnp.zeros((xs.shape[1] - C - 2 * E, T), jnp.float32))
        coded = jnp.concatenate(coded, axis=0)
        xs[rows(si, T, T), C:] = coded.T.astype(jnp.bfloat16)

    def normalize():
        def chunk(i):
            at = rows(i, 16, 16)
            x = tokv[at, :].astype(jnp.float32)
            scale = lax.rsqrt(jnp.mean(x * x, axis=1, keepdims=True) + norm_eps)
            mine = tokv[at, rows(ti, C, C)].astype(jnp.float32)
            to = pl.ds(pl.multiple_of(si * T + i * 16, 16), 16)
            xs[to, 0:C] = (mine * scale).astype(jnp.bfloat16)

        each(0, T // 16, chunk)

    def fold(m):
        def one(k):
            d = fs_peer(k)
            value = wf[m, d]
            if m < 2:
                value = value * gain[...]
            value = value.astype(jnp.bfloat16)

            def keep():
                new[m][gi, rows(si, F, F), :] = value

            def away():
                wb[m, d] = value

            pl.when(k == 0)(keep)
            pl.when(k > 0)(away)

        each(0, S, one)

    def fold_shared(m):
        value = sf[m]
        if m < 2:
            value = value * gain[...]
        shn[m][rows(si, SF, SF), :] = value.astype(jnp.bfloat16)

    def w_copy(q, d, s):
        m, c, width = parts[q]
        return rdma(
            wb.at[m, d, :, pl.ds(c, width)],
            new[m].at[gi, rows(s, F, F), pl.ds(c, width)],
            w_send.at[q, d],
            w_recv.at[q, s],
            {"fs": d},
        )

    def spread(block, s, up, down, act_on):
        place, ssem, rsem, after = block
        at = place(s)

        def hop(way, dev):
            act_on(rdma(at, at, ssem.at[s, way], rsem.at[s], {"fs": dev}))

        if up:
            pl.when(zi < Z - 1)(lambda: hop(0, si + Y))
        if down:
            pl.when(zi > 0)(lambda: hop(1, si - Y))

        def across(k):
            y = lax.rem(yi + k, Y)
            hop(2 + y, zi * Y + y)

        each(1, Y, across)

    def shx_copy(m, s, g, dev):
        at = sh_place(m, s, g)
        return rdma(at, at, shx_send.at[m, s, dev], shx_recv.at[m, s, g], {"gr": dev})

    def arrive(block, s):
        place, ssem, rsem, after = block
        rdma(place(s), place(s), ssem.at[s, 0], rsem.at[s], {"fs": fs_peer(1)}).wait_recv()
        if after is not None:
            after(s)

    def start(c):
        c.start()

    def sent(c):
        c.wait_send()

    def relay(block, step, act_on=start):
        def from_below():
            s = si - step * Y
            if act_on is start:
                arrive(block, s)
            spread(block, s, True, False, act_on)

        def from_above():
            s = si + step * Y
            if act_on is start:
                arrive(block, s)
            spread(block, s, False, True, act_on)

        pl.when(zi >= step)(from_below)
        pl.when(zi + step < Z)(from_above)

    def others_arrive(block, step):
        def at(z):
            each(1, Y, lambda k: arrive(block, z * Y + lax.rem(yi + k, Y)))

        if step == 0:
            at(zi)
        else:
            pl.when(zi >= step)(lambda: at(zi - step))
            pl.when(zi + step < Z)(lambda: at(zi + step))

    def block_sent(block):
        spread(block, si, True, True, sent)
        for step in range(1, Z):
            relay(block, step, sent)

    def sh_place(m, s, g):
        return shn[m].at[rows(s, SF, SF), rows(g, C // G, C // G)]

    def sh_block(m):
        return (
            lambda s: sh_place(m, s, gi),
            sh_send.at[m],
            sh_recv.at[m],
            lambda s: each(1, G, lambda j: shx_copy(m, s, gi, gr_peer(j)).start()),
        )

    tok_block = (lambda s: xs.at[rows(s, T, T)], tok_send, tok_recv, None)
    sh_blocks = [sh_block(m) for m in range(3)]

    def sh_hop(block, s, way, dev, act_on):
        place, ssem, rsem, after = block
        act_on(rdma(place(s), place(s), ssem.at[s, way], rsem.at[s], {"fs": dev}))

    def sh_along(block, s, up, down, act_on):
        if up:
            pl.when(zi < Z - 1)(lambda: sh_hop(block, s, 0, si + Y, act_on))
        if down:
            pl.when(zi > 0)(lambda: sh_hop(block, s, 1, si - Y, act_on))

    def sh_own(block, act_on):
        def across(k):
            y = lax.rem(yi + k, Y)
            sh_hop(block, si, 2 + y, zi * Y + y, act_on)

        each(1, Y, across)
        sh_along(block, si, True, True, act_on)

    def sh_relay(block, step, act_on):
        def one(s, up, down):
            if act_on is start:
                arrive(block, s)
            sh_along(block, s, up, down, act_on)

        if step == 0:
            each(1, Y, lambda k: one(zi * Y + lax.rem(yi + k, Y), True, True))
            return

        def row(z, up):
            each(0, Y, lambda k: one(z * Y + lax.rem(yi + k, Y), up, not up))

        pl.when(zi >= step)(lambda: row(zi - step, True))
        pl.when(zi + step < Z)(lambda: row(zi + step, False))

    def sh_sent(block):
        sh_own(block, sent)
        for step in range(Z):
            sh_relay(block, step, sent)

    def x_copy(q, s, g, dev):
        m, c, width = parts[q]
        place = new[m].at[g, rows(s, F, F), pl.ds(c, width)]
        return rdma(place, place, x_send.at[q, s, dev], x_recv.at[q, s, g], {"gr": dev})

    def send_weight(q):
        each(1, S, lambda k: w_copy(q, fs_peer(k), si).start())

    def send_own(q):
        each(1, G, lambda j: x_copy(q, si, gi, gr_peer(j)).start())

    def forward(m, lo=1, hi=S):
        def one(k):
            s = fs_from(k)
            w_copy(m, s, s).wait_recv()
            each(1, G, lambda j: x_copy(m, s, gi, gr_peer(j)).start())

        each(lo, hi, one)

    def x_arrive(m, g):
        each(0, S, lambda s: x_copy(m, s, g, g).wait_recv())

    def p_copy(j, t, s):
        return rdma(
            pout.at[j if slots > 1 else 0, t], pin.at[j, s], p_send.at[j, t], p_recv.at[j, s], {"tp": t}
        )

    def a_copy(j, t, s):
        place = act.at[j, rows(s, NH, NH)]
        return rdma(place, place, a_send.at[j, t], a_recv.at[j, s], {"tp": t})

    def first_matmuls(j):
        g = gr_peer(j)
        slot = j if slots > 1 else 0
        for q in range(TP):
            t = tp_peer(1 + q)

            def block(b, t=t):
                x = xs[rows(t * NB + b, T, T), 0:C]
                for m in range(2):
                    part = lax.dot_general(
                        x, new[m][g], (((1,), (1,)), ((), ())), preferred_element_type=jnp.float32
                    )
                    pout[slot, t, rows(b, T, T), m * H : (m + 1) * H] = part.astype(jnp.bfloat16)

            each(0, NB, block)
            if q < TP - 1:
                p_copy(j, t, ti).start()

    def activations(j):
        g = gr_peer(j)
        slot = j if slots > 1 else 0
        expert = g * S + si
        for q in range(1, TP):
            t = tp_peer(q)
            p_copy(j, t, t).wait_recv()

        def block(b):
            r = rows(b, T, T)
            pre = pout[slot, ti, r, :].astype(jnp.float32)
            for q in range(1, TP):
                pre = pre + pin[j, tp_peer(q), r, :].astype(jnp.float32)
            at = rows(ti * NB + b, T, T)
            coded = xs[at, C:].astype(jnp.float32)
            lane = lax.broadcasted_iota(jnp.int32, coded.shape, 1)
            share = jnp.sum(
                jnp.where((lane == expert) | (lane == expert + E), coded, 0.0), axis=1, keepdims=True
            )
            value = silu(pre[:, :H]) * pre[:, H:] * share
            act[j, at, :] = value.astype(jnp.bfloat16)

        each(0, NB, block)
        for q in range(1, TP):
            a_copy(j, tp_peer(q), ti).start()

    def p_copy(j, t, s, place):
        return rdma(
            pout.at[j if slots > 1 else 0, t],
            pin.at[j, place],
            p_send.at[j, t],
            p_recv.at[j, s],
            {"tp": t},
        )

    def a_copy(j, t, s):
        place = act.at[j, rows(s, NH, NH)]
        return rdma(place, place, a_send.at[j, t], a_recv.at[j, s], {"tp": t})

    PB = 2 if NB % 2 == 0 else 1

    def first_matmuls(j):
        g = gr_peer(j)
        slot = j if slots > 1 else 0
        for q in range(TP):
            t = tp_peer(1 + q)

            def block(b, t=t):
                x = xs[pl.ds(pl.multiple_of((t * NB + b * PB) * T, T), PB * T), 0:C]
                for m in range(2):
                    part = lax.dot_general(
                        x, new[m][g], (((1,), (1,)), ((), ())), preferred_element_type=jnp.float32
                    )
                    at = pl.ds(pl.multiple_of(b * PB * T, T), PB * T)
                    pout[slot, t, at, m * H : (m + 1) * H] = part.astype(jnp.bfloat16)

            each(0, NB // PB, block)
            if q < TP - 1:
                p_copy(j, t, ti, TP - 2 - q).start()

    def activations(j):
        g = gr_peer(j)
        slot = j if slots > 1 else 0
        expert = g * S + si
        for q in range(1, TP):
            t = tp_peer(q)
            p_copy(j, t, t, q - 1).wait_recv()

        def block(b):
            r = rows(b, T, T)
            pre = pout[slot, ti, r, :].astype(jnp.float32)
            for q in range(1, TP):
                pre = pre + pin[j, q - 1, r, :].astype(jnp.float32)
            at = rows(ti * NB + b, T, T)
            coded = xs[at, C:].astype(jnp.float32)
            lane = lax.broadcasted_iota(jnp.int32, coded.shape, 1)
            share = jnp.sum(
                jnp.where((lane == expert) | (lane == expert + E), coded, 0.0), axis=1, keepdims=True
            )
            value = silu(pre[:, :H]) * pre[:, H:] * share
            act[j, at, :] = value.astype(jnp.bfloat16)

        each(0, NB, block)
        for q in range(1, TP):
            a_copy(j, tp_peer(q), ti).start()

    def x_arrive(q, g):
        each(0, S, lambda s: x_copy(q, s, g, g).wait_recv())

    def piece(p):
        return pl.ds(p * CW, CW)

    def ry_copy(p, z, y, src):
        return rdma(
            oz.at[rows(z * Y + y, T, T), piece(p)],
            rety.at[p, z, src],
            ry_send.at[p, z, y],
            ry_recv.at[p, z, src],
            {"fs": zi * Y + y},
        )

    def r_copy(p, z, y, col, up, dist):
        slot = Z if dist == 1 and not up else z
        return rdma(
            oz.at[rows(z * Y + y, T, T), piece(p)],
            ret.at[p, col, slot],
            r_send.at[p, col, z],
            r_recv.at[p, col, slot],
            {"fs": si + Y if up else si - Y},
        )

    def far_first(fn):
        for dist in range(Z - 1, -1, -1):
            pl.when(zi + dist < Z)(functools.partial(fn, zi + dist, True, dist))
            if dist:
                pl.when(zi >= dist)(functools.partial(fn, zi - dist, False, dist))

    def down(p):
        def block(z, up, dist):
            def column(k):
                y = lax.rem(yi + k, Y)
                at = rows(z * Y + y, T, T)
                total = jnp.zeros((T, CW), jnp.float32)
                for j in range(G):
                    total = total + jnp.dot(
                        act[j, at, :], new[2][gr_peer(j), :, piece(p)], preferred_element_type=jnp.float32
                    )
                oz[at, piece(p)] = total.astype(jnp.bfloat16)
                if modes[p] == "A":
                    pl.when(y != yi)(lambda: ry_copy(p, z, y, yi).start())
                elif dist:
                    ends = zi == 0 if up else zi == Z - 1
                    pl.when(ends)(lambda: r_copy(p, z, y, y, up, dist).start())

            each(1, Y + 1, column)

        far_first(block)

    def chain(p, z, y, col, up, dist, final=False):
        at = rows(z * Y + y, T, T)

        def add_far(slot):
            rdma(
                ret.at[p, col, slot],
                ret.at[p, col, slot],
                r_send.at[p, col, z],
                r_recv.at[p, col, slot],
                {"fs": fs_peer(1)},
            ).wait_recv()
            total = oz[at, piece(p)].astype(jnp.float32) + ret[p, col, slot].astype(jnp.float32)
            oz[at, piece(p)] = total.astype(jnp.bfloat16)

        inner = True
        if dist == 0 or up:
            inner = zi > 0
            pl.when(zi > 0)(lambda: add_far(z))
        if dist == 0:
            pl.when(zi < Z - 1)(lambda: add_far(Z))
        elif not up:
            inner = zi < Z - 1
            pl.when(zi < Z - 1)(lambda: add_far(z))
        if dist:
            if modes[p] == "A":
                r_copy(p, z, y, col, up, dist).start()
            else:
                pl.when(inner)(lambda: r_copy(p, z, y, col, up, dist).start())

    def across_sum(p, z):
        at = rows(z * Y + yi, T, T)
        total = oz[at, piece(p)].astype(jnp.float32)
        for k in range(1, Y):
            y = lax.rem(yi + k, Y)
            ry_copy(p, z, y, y).wait_recv()
            total = total + rety[p, z, y].astype(jnp.float32)
        oz[at, piece(p)] = total.astype(jnp.bfloat16)

    def gather_far(p):
        def block(z, up, dist):
            if modes[p] == "A":
                across_sum(p, z)
                chain(p, z, yi, 0, up, dist)
                return

            def column(k):
                y = lax.rem(yi + k, Y)
                chain(p, z, y, y, up, dist)
                if dist == 0:
                    pl.when(y != yi)(lambda: ry_copy(p, z, y, yi).start())

            each(1, Y + 1, column)

        far_first(block)

    def gather_near(p):
        if modes[p] == "B":
            across_sum(p, zi)

    def return_sent(p):
        def block(z, up, dist):
            def column(k):
                y = lax.rem(yi + k, Y)
                if modes[p] == "A":
                    pl.when(y != yi)(lambda: ry_copy(p, z, y, yi).wait_send())
                    if dist:
                        pl.when(y == yi)(lambda: r_copy(p, z, y, 0, up, dist).wait_send())
                elif dist:
                    r_copy(p, z, y, y, up, dist).wait_send()
                else:
                    pl.when(y != yi)(lambda: ry_copy(p, z, y, yi).wait_send())

            each(1, Y + 1, column)

        far_first(block)

    def shared_arrive(m):
        each(
            1,
            S,
            lambda k: each(
                1, G, lambda j: shx_copy(m, fs_from(k), gr_peer(j), gr_peer(j)).wait_recv()
            ),
        )

    def ps_copy(t, s):
        return rdma(psh, pshin.at[s], ps_send.at[t], ps_recv.at[s], {"tp": t})

    def shared_first(m):
        part = lax.dot_general(
            xs[rows(si, T, T), 0:C],
            shn[m][...],
            (((1,), (1,)), ((), ())),
            preferred_element_type=jnp.float32,
        )
        psh[:, m * SH : (m + 1) * SH] = part.astype(jnp.bfloat16)

    def act_arrive():
        for q in range(1, TP):
            for j in range(G):
                a_copy(j, tp_peer(q), tp_peer(q)).wait_recv()

    scope = jax.named_scope

    def span(text):
        q, lo, hi = (text + ":0:8").split(":")[:3]
        return int(q), max(1, int(lo) * S // 8), int(hi) * S // 8

    def run(name):
        op, num = name[0], name[1:]
        with scope(name.replace(":", "_")):
            if op == "T":
                spread(tok_block, si, True, True, start)
            elif op == "B":
                pl.semaphore_wait(barrier, S + G + TP - 3)
            elif op == "C":
                m = int(num)
                inputs[1 + m].wait()
                fold(m)
            elif op == "c":
                for m in range(3):
                    inputs[4 + m].wait()
                    fold_shared(m)
            elif op == "X":
                send_own(int(num))
            elif op == "W":
                q, lo, hi = span(num)
                each(lo, hi, lambda k: w_copy(q, fs_peer(k), si).start())
            elif op == "R":
                relay(tok_block, int(num))
            elif op == "F":
                forward(*span(num))
            elif op == "O":
                others_arrive(tok_block, int(num))
            elif op == "S":
                for block in sh_blocks:
                    sh_own(block, start)
            elif op == "s":
                for block in sh_blocks:
                    sh_relay(block, int(num), start)
            elif op == "M":
                j = int(num)
                if slots == 1 and j > 0:
                    for q in range(1, TP):
                        p_copy(j - 1, tp_peer(q), ti, 0).wait_send()
                first_matmuls(j)
            elif op == "V":
                activations(int(num))
            elif op == "A":
                for j in range(1, G):
                    x_arrive(int(num), gr_peer(j))
            elif op == "a":
                act_arrive()
            elif op == "D":
                down(int(num))
            elif op == "G":
                gather_far(int(num))
            elif op == "H":
                for m in range(2):
                    shared_arrive(m)
                    shared_first(m)
                for q in range(1, TP):
                    ps_copy(tp_peer(q), ti).start()
            elif op == "P":
                shared_arrive(2)
                pre = psh[...].astype(jnp.float32)
                for q in range(1, TP):
                    t = tp_peer(q)
                    ps_copy(t, t).wait_recv()
                    pre = pre + pshin[t].astype(jnp.float32)
                shared_act = (silu(pre[:, :SH]) * pre[:, SH:]).astype(jnp.bfloat16)
                rest.append(jnp.dot(shared_act, shn[2][...], preferred_element_type=jnp.float32))
            elif op == "E":
                for p in range(pieces):
                    gather_near(p)
                total = rest[0] + oz[rows(si, T, T), :].astype(jnp.float32)
                mixed[...] = total.astype(jnp.bfloat16)
            else:
                raise ValueError(name)

    rest = []
    with scope("prologue"):
        route_codes()
        inputs[0].wait()
        normalize()
    for name in SCHEDULE:
        run(name)

    for q in range(len(parts)):
        each(1, S, lambda k, q=q: w_copy(q, fs_peer(k), si).wait_send())
        each(0, S, lambda s, q=q: each(1, G, lambda j: x_copy(q, s, gi, gr_peer(j)).wait_send()))
    for m in range(3):
        sh_sent(sh_blocks[m])
        each(
            1,
            S,
            lambda k, m=m: each(
                1, G, lambda j: shx_copy(m, fs_from(k), gi, gr_peer(j)).wait_send()
            ),
        )
    block_sent(tok_block)
    for p in range(pieces):
        return_sent(p)
    for q in range(1, TP):
        t = tp_peer(q)
        ps_copy(t, ti).wait_send()
        for j in range(G):
            if slots > 1 or j == G - 1:
                p_copy(j, t, ti, 0).wait_send()
            a_copy(j, t, ti).wait_send()


def emit_kernel(*refs):
    n = len(refs) // 2
    sem = refs[-1]
    copies = []
    for i in range(n):
        dst = refs[n + i]
        if len(dst.shape) == 4:
            dst = dst.at[:, 0]
        copies.append(pltpu.make_async_copy(refs[i], dst, sem.at[i]))
    for c in copies:
        c.start()
    for c in copies:
        c.wait()


def emit(results, G):
    bf16 = jnp.bfloat16
    shapes = [r.shape if len(r.shape) < 3 else (r.shape[0], 1) + r.shape[1:] for r in results]
    n = len(results)
    return pl.pallas_call(
        emit_kernel,
        out_shape=[jax.ShapeDtypeStruct(s, bf16) for s in shapes],
        in_specs=[pl.BlockSpec(memory_space=pltpu.VMEM)] * n,
        out_specs=[pl.BlockSpec(memory_space=pl.ANY)] * n,
        scratch_shapes=[pltpu.SemaphoreType.DMA((n,))],
        compiler_params=pltpu.CompilerParams(vmem_limit_bytes=vmem_bytes // 2),
        name="emit",
    )(*results)


def body(
    Y,
    tokens,
    expert_ids,
    route_weight,
    norm_gain,
    expert_gate,
    expert_up,
    expert_down,
    shared_gate,
    shared_up,
    shared_down,
):
    G, S, TP = lax.axis_size("gr"), lax.axis_size("fs"), lax.axis_size("tp")
    T, C = tokens.shape[0], expert_gate.shape[2]
    F, SF = expert_gate.shape[1], shared_gate.shape[0]
    H, SH = F * S, SF * S
    E, N = G * S, S * T
    NH = N // TP
    lanes = -(-2 * E // 128) * 128
    bf16, f32 = jnp.bfloat16, jnp.float32
    halves = 1 if C % 256 == 0 and C >= 1024 else 1
    modes = "A" if C % 512 == 0 and C >= 1024 else "A"
    P = len(modes)
    columns = Y if "B" in modes else 1
    Q = 2 + halves

    out_bytes = 2 * C * (T + 3 * G * H + 3 * SH)
    limit = vmem_bytes - 5 * out_bytes // 4
    fixed = 2 * (N * (3 * C + lanes + G * H) + T * (columns * (S // Y + 1) * C + 2 * SH * (TP + 1)))
    fixed += 6 * 3 * S * F * C + 4 * 3 * SF * C + 2 * T * tokens.shape[1] + 2 * N * G * 2 * H
    slots = G if fixed + 2 * N * G * 2 * H < limit - (1 << 21) else 1
    dims = (G, S, TP, T, C, H, F, SF, slots, Y, halves, modes)
    vmem, hbm = pl.BlockSpec(memory_space=pltpu.VMEM), pl.BlockSpec(memory_space=pl.ANY)
    dma = pltpu.SemaphoreType.DMA
    results = pl.pallas_call(
        functools.partial(handover, dims),
        out_shape=[pltpu.VMEM((T, C), bf16)]
        + [pltpu.VMEM((G, H, C), bf16)] * 3
        + [pltpu.VMEM((SH, C), bf16)] * 3,
        in_specs=[hbm, vmem, vmem, vmem] + [hbm] * 6,
        out_specs=[vmem] * 7,
        scratch_shapes=[
            pltpu.VMEM(tokens.shape, bf16),
            pltpu.VMEM((3, S, F, C), f32),
            pltpu.VMEM((3, SF, C), f32),
            pltpu.VMEM((3, S, F, C), bf16),
            pltpu.VMEM((N, C + lanes), bf16),
            pltpu.VMEM((slots, TP, NH, 2 * H), bf16),
            pltpu.VMEM((G, max(TP - 1, 1), NH, 2 * H), bf16),
            pltpu.VMEM((G, N, H), bf16),
            pltpu.VMEM((N, C), bf16),
            pltpu.VMEM((P, S // Y, Y, T, C // P), bf16),
            pltpu.VMEM((P, columns, S // Y + 1, T, C // P), bf16),
            pltpu.VMEM((T, 2 * SH), bf16),
            pltpu.VMEM((TP, T, 2 * SH), bf16),
            dma((7,)),
            dma((S, 2 + Y)),
            dma((S,)),
            dma((Q, S)),
            dma((Q, S)),
            dma((Q, S, G)),
            dma((Q, S, G)),
            dma((3, S, 2 + Y)),
            dma((3, S)),
            dma((3, S, G)),
            dma((3, S, G)),
            dma((G, TP)),
            dma((G, TP)),
            dma((G, TP)),
            dma((G, TP)),
            dma((P, S // Y, Y)),
            dma((P, S // Y, Y)),
            dma((P, columns, S // Y)),
            dma((P, columns, S // Y + 1)),
            dma((TP,)),
            dma((TP,)),
        ],
        compiler_params=pltpu.CompilerParams(
            collective_id=0, has_side_effects=True, vmem_limit_bytes=limit
        ),
        name="handover",
    )(
        tokens,
        expert_ids.T,
        route_weight.T,
        norm_gain[None],
        expert_gate,
        expert_up,
        expert_down,
        shared_gate,
        shared_up,
        shared_down,
    )
    return emit(results, G)


def line_length(mesh):
    places = [d.coords for d in mesh.devices[0, :, 0]]
    axis = [i for i in range(3) if places[0][i] != places[1][i]][0]
    count = 0
    for place in places:
        if any(place[i] != places[0][i] for i in range(3) if i != axis):
            break
        count += 1
    return count if len(places) % count == 0 else len(places)


def solution(mesh):
    placed = (
        P(("gr", "fs"), None),
        P(("gr", "fs"), None),
        P(("gr", "fs"), None),
        P("tp"),
        P("gr", "fs", "tp"),
        P("gr", "fs", "tp"),
        P("gr", "fs", "tp"),
        P("fs", "tp"),
        P("fs", "tp"),
        P("fs", "tp"),
    )
    return jax.shard_map(
        functools.partial(body, line_length(mesh)),
        mesh=mesh,
        in_specs=placed,
        out_specs=(
            P(("gr", "fs"), "tp"),
            P(None, "fs", None, "tp"),
            P(None, "fs", None, "tp"),
            P(None, "fs", None, "tp"),
            P(None, "tp"),
            P(None, "tp"),
            P(None, "tp"),
        ),
        check_vma=False,
    )
```

```python
import functools

import jax
import jax.numpy as jnp
from jax import lax
from jax.experimental import pallas as pl
from jax.experimental.pallas import tpu as pltpu
from jax.sharding import PartitionSpec as P

SCHEDULE = ('B', 'T', 'C0', 'X0', 'W001', 'C1', 'C2', 'c', 'X1', 'X2', 'W10', 'W20', 'R1', 'W023', 'F00', 'F01', 'F10', 'F20', 'R2', 'W11', 'F02', 'F03', 'R3', 'W123', 'F11', 'W2123', 'F12', 'F13', 'S', 'O0', 'O1', 'O2', 'O3', 'M0', 'F21', 'F22', 'F23', 'V0', 'A0', 'A1', 's0', 'M1', 'V1', 's1', 'A2', 'a', 'D0', 's2', 'G0:3', 'wT01', 's3', 'G0:2', 'w2Ps', 'G0:1', 'H', 'P', 'wS', 'G0:0', 'E', 'wRp')
route_scale = 2.5
norm_eps = 1e-06
vmem_bytes = 67043328


def fold_gain(weight, gain):
    return (weight * gain).astype(jnp.bfloat16)


def silu(v):
    return v / (1.0 + jnp.exp(-v))


def handover(
    dims,
    tok,
    ids,
    scores,
    gain,
    w0,
    w1,
    w2,
    s0,
    s1,
    s2,
    mixed,
    n0,
    n1,
    n2,
    hs,
    tokv,
    wf,
    sf,
    wb,
    xs,
    pout,
    pin,
    act,
    oz,
    rety,
    ret,
    psh,
    pshin,
    in_sem,
    tok_send,
    tok_recv,
    w_send,
    w_recv,
    x_send,
    x_recv,
    sh_send,
    sh_recv,
    shx_send,
    shx_recv,
    p_send,
    p_recv,
    a_send,
    a_recv,
    ry_send,
    ry_recv,
    r_send,
    r_recv,
    ps_send,
    ps_recv,
):
    G, S, TP, T, C, H, F, SF, slots, Y, halves, modes = dims
    Z = S // Y
    E = G * S
    SH = SF * S
    NB = S // TP
    NH = NB * T
    gi, si, ti = lax.axis_index("gr"), lax.axis_index("fs"), lax.axis_index("tp")
    zi, yi = si // Y, lax.rem(si, Y)
    w, new, sh = (w0, w1, w2), (n0, n1, n2), (s0, s1, s2)
    HW, pieces = C // halves, len(modes)
    CW = C // pieces
    parts = [(0, 0, C), (1, 0, C)] + [(2, h * HW, HW) for h in range(halves)]

    def rdma(src, dst, ssem, rsem, dev):
        return pltpu.make_async_remote_copy(
            src_ref=src,
            dst_ref=dst,
            send_sem=ssem,
            recv_sem=rsem,
            device_id=dev,
            device_id_type=pl.DeviceIdType.MESH,
        )

    def rows(start, step, size):
        return pl.ds(pl.multiple_of(start * step, step), size)

    def each(lo, hi, fn):
        def step(i, c):
            fn(i)
            return c

        lax.fori_loop(lo, hi, step, 0)

    def fs_peer(k):
        return lax.rem(si + k, S)

    def fs_from(k):
        return lax.rem(si + S - k, S)

    def gr_peer(k):
        return lax.rem(gi + k, G)

    def tp_peer(k):
        return lax.rem(ti + k, TP)

    barrier = pltpu.get_barrier_semaphore()

    def greet(axis, peer, n):
        each(
            1,
            n,
            lambda k: pl.semaphore_signal(
                barrier,
                inc=1,
                device_id={axis: peer(k)},
                device_id_type=pl.DeviceIdType.MESH,
            ),
        )

    greet("fs", fs_peer, S)
    greet("gr", gr_peer, G)
    greet("tp", tp_peer, TP)
    inputs = [
        pltpu.make_async_copy(tok, tokv, in_sem.at[0]),
        *(pltpu.make_async_copy(w[m], wf.at[m], in_sem.at[1 + m]) for m in range(3)),
        *(pltpu.make_async_copy(sh[m], sf.at[m], in_sem.at[4 + m]) for m in range(3)),
    ]
    for copy in inputs:
        copy.start()

    def route_codes():
        share = scores[...] / jnp.sum(scores[...], axis=0, keepdims=True) * route_scale
        expert = lax.broadcasted_iota(jnp.int32, (E, T), 0)
        dense = jnp.zeros((E, T), jnp.float32)
        for k in range(ids.shape[0]):
            dense = dense + jnp.where(expert == ids[k : k + 1, :], share[k : k + 1, :], 0.0)
        high = dense.astype(jnp.bfloat16).astype(jnp.float32)
        coded = [high, dense - high]
        if C + 2 * E < xs.shape[1]:
            coded.append(jnp.zeros((xs.shape[1] - C - 2 * E, T), jnp.float32))
        coded = jnp.concatenate(coded, axis=0)
        xs[rows(si, T, T), C:] = coded.T.astype(jnp.bfloat16)

    def normalize():
        def chunk(i):
            at = rows(i, 16, 16)
            x = tokv[at, :].astype(jnp.float32)
            scale = lax.rsqrt(jnp.mean(x * x, axis=1, keepdims=True) + norm_eps)
            mine = tokv[at, rows(ti, C, C)].astype(jnp.float32)
            to = pl.ds(pl.multiple_of(si * T + i * 16, 16), 16)
            xs[to, 0:C] = (mine * scale).astype(jnp.bfloat16)

        each(0, T // 16, chunk)

    def fold(m):
        def one(k):
            d = fs_peer(k)
            value = wf[m, d]
            if m < 2:
                value = value * gain[...]
            value = value.astype(jnp.bfloat16)

            def keep():
                new[m][gi, rows(si, F, F), :] = value

            def away():
                wb[m, d] = value

            pl.when(k == 0)(keep)
            pl.when(k > 0)(away)

        each(0, S, one)

    def fold_shared(m):
        value = sf[m]
        if m < 2:
            value = value * gain[...]
        hs[m, rows(si, SF, SF), :] = value.astype(jnp.bfloat16)

    def w_copy(q, d, s):
        m, c, width = parts[q]
        return rdma(
            wb.at[m, d, :, pl.ds(c, width)],
            new[m].at[gi, rows(s, F, F), pl.ds(c, width)],
            w_send.at[q],
            w_recv.at[q, s],
            {"fs": d},
        )

    def spread(block, s, up, down, act_on):
        place, ssem, rsem, after = block
        at = place(s)

        def hop(way, dev):
            act_on(rdma(at, at, ssem.at[s, way], rsem.at[s], {"fs": dev}))

        if up:
            pl.when(zi < Z - 1)(lambda: hop(0, si + Y))
        if down:
            pl.when(zi > 0)(lambda: hop(1, si - Y))

        def across(k):
            y = lax.rem(yi + k, Y)
            hop(2 + y, zi * Y + y)

        each(1, Y, across)

    def sh_place(s, g):
        return hs.at[:, rows(s, SF, SF), rows(g, C // G, C // G)]

    def shx_copy(s, g, dev):
        at = sh_place(s, g)
        return rdma(at, at, shx_send.at[dev], shx_recv.at[g], {"gr": dev})

    def arrive(block, s):
        place, ssem, rsem, after = block
        rdma(place(s), place(s), ssem.at[s, 0], rsem.at[s], {"fs": fs_peer(1)}).wait_recv()
        if after is not None:
            after(s)

    def start(c):
        c.start()

    def sent(c):
        c.wait_send()

    def relay(block, step, act_on=start):
        def from_below():
            s = si - step * Y
            if act_on is start:
                arrive(block, s)
            spread(block, s, True, False, act_on)

        def from_above():
            s = si + step * Y
            if act_on is start:
                arrive(block, s)
            spread(block, s, False, True, act_on)

        pl.when(zi >= step)(from_below)
        pl.when(zi + step < Z)(from_above)

    def others_arrive(block, step):
        def at(z):
            each(1, Y, lambda k: arrive(block, z * Y + lax.rem(yi + k, Y)))

        if step == 0:
            at(zi)
        else:
            pl.when(zi >= step)(lambda: at(zi - step))
            pl.when(zi + step < Z)(lambda: at(zi + step))

    def block_sent(block):
        spread(block, si, True, True, sent)
        for step in range(1, Z):
            relay(block, step, sent)

    sh_block = (
        lambda s: sh_place(s, gi),
        sh_send,
        sh_recv,
        lambda s: each(1, G, lambda j: shx_copy(s, gi, gr_peer(j)).start()),
    )
    tok_block = (lambda s: xs.at[rows(s, T, T)], tok_send, tok_recv, None)

    def sh_hop(block, s, way, dev, act_on):
        place, ssem, rsem, after = block
        act_on(rdma(place(s), place(s), ssem.at[s, way], rsem.at[s], {"fs": dev}))

    def sh_along(block, s, up, down, act_on):
        if up:
            pl.when(zi < Z - 1)(lambda: sh_hop(block, s, 0, si + Y, act_on))
        if down:
            pl.when(zi > 0)(lambda: sh_hop(block, s, 1, si - Y, act_on))

    def sh_own(block, act_on):
        def across(k):
            y = lax.rem(yi + k, Y)
            sh_hop(block, si, 2 + y, zi * Y + y, act_on)

        each(1, Y, across)
        sh_along(block, si, True, True, act_on)

    def sh_relay(block, step, act_on):
        def one(s, up, down):
            if act_on is start:
                arrive(block, s)
            sh_along(block, s, up, down, act_on)

        if step == 0:
            each(1, Y, lambda k: one(zi * Y + lax.rem(yi + k, Y), True, True))
            return

        def row(z, up):
            each(0, Y, lambda k: one(z * Y + lax.rem(yi + k, Y), up, not up))

        pl.when(zi >= step)(lambda: row(zi - step, True))
        pl.when(zi + step < Z)(lambda: row(zi + step, False))

    def sh_sent(block):
        sh_own(block, sent)
        for step in range(Z):
            sh_relay(block, step, sent)

    def x_copy(q, s, g, dev):
        m, c, width = parts[q]
        place = new[m].at[g, rows(s, F, F), pl.ds(c, width)]
        return rdma(place, place, x_send.at[q, dev], x_recv.at[q, g], {"gr": dev})

    def send_own(q):
        each(1, G, lambda j: x_copy(q, si, gi, gr_peer(j)).start())

    def p_copy(j, t, s):
        return rdma(
            pout.at[j if slots > 1 else 0, t], pin.at[j, s], p_send.at[j, t], p_recv.at[j, s], {"tp": t}
        )

    def a_copy(j, t, s):
        place = act.at[j, rows(s, NH, NH)]
        return rdma(place, place, a_send.at[j, t], a_recv.at[j, s], {"tp": t})

    def first_matmuls(j):
        g = gr_peer(j)
        slot = j if slots > 1 else 0
        for q in range(TP):
            t = tp_peer(1 + q)

            def block(b, t=t):
                x = xs[rows(t * NB + b, T, T), 0:C]
                for m in range(2):
                    part = lax.dot_general(
                        x, new[m][g], (((1,), (1,)), ((), ())), preferred_element_type=jnp.float32
                    )
                    pout[slot, t, rows(b, T, T), m * H : (m + 1) * H] = part.astype(jnp.bfloat16)

            each(0, NB, block)
            if q < TP - 1:
                p_copy(j, t, ti).start()

    def activations(j):
        g = gr_peer(j)
        slot = j if slots > 1 else 0
        expert = g * S + si
        for q in range(1, TP):
            t = tp_peer(q)
            p_copy(j, t, t).wait_recv()

        def block(b):
            r = rows(b, T, T)
            pre = pout[slot, ti, r, :].astype(jnp.float32)
            for q in range(1, TP):
                pre = pre + pin[j, tp_peer(q), r, :].astype(jnp.float32)
            at = rows(ti * NB + b, T, T)
            coded = xs[at, C:].astype(jnp.float32)
            lane = lax.broadcasted_iota(jnp.int32, coded.shape, 1)
            share = jnp.sum(
                jnp.where((lane == expert) | (lane == expert + E), coded, 0.0), axis=1, keepdims=True
            )
            value = silu(pre[:, :H]) * pre[:, H:] * share
            act[j, at, :] = value.astype(jnp.bfloat16)

        each(0, NB, block)
        for q in range(1, TP):
            a_copy(j, tp_peer(q), ti).start()

    def p_copy(j, t, s, place):
        return rdma(
            pout.at[j if slots > 1 else 0, t],
            pin.at[j, place],
            p_send.at[j, t],
            p_recv.at[j, s],
            {"tp": t},
        )

    def a_copy(j, t, s):
        place = act.at[j, rows(s, NH, NH)]
        return rdma(place, place, a_send.at[j, t], a_recv.at[j, s], {"tp": t})

    PB = 2 if NB % 2 == 0 else 1

    def first_matmuls(j):
        g = gr_peer(j)
        slot = j if slots > 1 else 0
        for q in range(TP):
            t = tp_peer(1 + q)

            def block(b, t=t):
                x = xs[pl.ds(pl.multiple_of((t * NB + b * PB) * T, T), PB * T), 0:C]
                for m in range(2):
                    part = lax.dot_general(
                        x, new[m][g], (((1,), (1,)), ((), ())), preferred_element_type=jnp.float32
                    )
                    at = pl.ds(pl.multiple_of(b * PB * T, T), PB * T)
                    pout[slot, t, at, m * H : (m + 1) * H] = part.astype(jnp.bfloat16)

            each(0, NB // PB, block)
            if q < TP - 1:
                p_copy(j, t, ti, TP - 2 - q).start()

    def activations(j):
        g = gr_peer(j)
        slot = j if slots > 1 else 0
        expert = g * S + si
        for q in range(1, TP):
            t = tp_peer(q)
            p_copy(j, t, t, q - 1).wait_recv()

        def block(b):
            r = rows(b, T, T)
            pre = pout[slot, ti, r, :].astype(jnp.float32)
            for q in range(1, TP):
                pre = pre + pin[j, q - 1, r, :].astype(jnp.float32)
            at = rows(ti * NB + b, T, T)
            coded = xs[at, C:].astype(jnp.float32)
            lane = lax.broadcasted_iota(jnp.int32, coded.shape, 1)
            share = jnp.sum(
                jnp.where((lane == expert) | (lane == expert + E), coded, 0.0), axis=1, keepdims=True
            )
            value = silu(pre[:, :H]) * pre[:, H:] * share
            act[j, at, :] = value.astype(jnp.bfloat16)

        each(0, NB, block)
        for q in range(1, TP):
            a_copy(j, tp_peer(q), ti).start()

    def x_whole(q, g, dev):
        m, c, width = parts[q]
        place = new[m].at[g, :, pl.ds(c, width)]
        return rdma(place, place, x_send.at[q, dev], x_recv.at[q, g], {"gr": dev})

    def x_arrive(q, g):
        x_whole(q, g, g).wait_recv()

    def piece(p):
        return pl.ds(p * CW, CW)

    def ry_copy(p, z, y, src):
        return rdma(
            oz.at[rows(z * Y + y, T, T), piece(p)],
            rety.at[p, z, src],
            ry_send.at[p, z, y],
            ry_recv.at[p, z, src],
            {"fs": zi * Y + y},
        )

    def r_copy(p, z, y, col, up, dist):
        slot = Z if dist == 1 and not up else z
        return rdma(
            oz.at[rows(z * Y + y, T, T), piece(p)],
            ret.at[p, col, slot],
            r_send.at[p, col, z],
            r_recv.at[p, col, slot],
            {"fs": si + Y if up else si - Y},
        )

    def far_first(fn, only=None):
        for dist in range(Z - 1, -1, -1):
            if only is not None and dist != only:
                continue
            pl.when(zi + dist < Z)(functools.partial(fn, zi + dist, True, dist))
            if dist:
                pl.when(zi >= dist)(functools.partial(fn, zi - dist, False, dist))

    def down(p):
        def block(z, up, dist):
            def column(k):
                y = lax.rem(yi + k, Y)
                at = rows(z * Y + y, T, T)
                total = jnp.zeros((T, CW), jnp.float32)
                for j in range(G):
                    total = total + jnp.dot(
                        act[j, at, :], new[2][gr_peer(j), :, piece(p)], preferred_element_type=jnp.float32
                    )
                oz[at, piece(p)] = total.astype(jnp.bfloat16)
                if modes[p] == "A":
                    pl.when(y != yi)(lambda: ry_copy(p, z, y, yi).start())
                elif dist:
                    ends = zi == 0 if up else zi == Z - 1
                    pl.when(ends)(lambda: r_copy(p, z, y, y, up, dist).start())

            each(1, Y + 1, column)

        far_first(block)

    def chain(p, z, y, col, up, dist, final=False):
        at = rows(z * Y + y, T, T)

        def add_far(slot):
            rdma(
                ret.at[p, col, slot],
                ret.at[p, col, slot],
                r_send.at[p, col, z],
                r_recv.at[p, col, slot],
                {"fs": fs_peer(1)},
            ).wait_recv()
            total = oz[at, piece(p)].astype(jnp.float32) + ret[p, col, slot].astype(jnp.float32)
            oz[at, piece(p)] = total.astype(jnp.bfloat16)

        inner = True
        if dist == 0 or up:
            inner = zi > 0
            pl.when(zi > 0)(lambda: add_far(z))
        if dist == 0:
            pl.when(zi < Z - 1)(lambda: add_far(Z))
        elif not up:
            inner = zi < Z - 1
            pl.when(zi < Z - 1)(lambda: add_far(z))
        if dist:
            if modes[p] == "A":
                r_copy(p, z, y, col, up, dist).start()
            else:
                pl.when(inner)(lambda: r_copy(p, z, y, col, up, dist).start())

    def across_sum(p, z):
        at = rows(z * Y + yi, T, T)
        total = oz[at, piece(p)].astype(jnp.float32)
        for k in range(1, Y):
            y = lax.rem(yi + k, Y)
            ry_copy(p, z, y, y).wait_recv()
            total = total + rety[p, z, y].astype(jnp.float32)
        oz[at, piece(p)] = total.astype(jnp.bfloat16)

    def gather_far(p, only=None):
        def block(z, up, dist):
            if modes[p] == "A":
                across_sum(p, z)
                chain(p, z, yi, 0, up, dist)
                return

            def column(k):
                y = lax.rem(yi + k, Y)
                chain(p, z, y, y, up, dist)
                if dist == 0:
                    pl.when(y != yi)(lambda: ry_copy(p, z, y, yi).start())

            each(1, Y + 1, column)

        far_first(block, only)

    def gather_near(p):
        if modes[p] == "B":
            across_sum(p, zi)

    def return_sent(p):
        def block(z, up, dist):
            def column(k):
                y = lax.rem(yi + k, Y)
                if modes[p] == "A":
                    pl.when(y != yi)(lambda: ry_copy(p, z, y, yi).wait_send())
                    if dist:
                        pl.when(y == yi)(lambda: r_copy(p, z, y, 0, up, dist).wait_send())
                elif dist:
                    r_copy(p, z, y, y, up, dist).wait_send()
                else:
                    pl.when(y != yi)(lambda: ry_copy(p, z, y, yi).wait_send())

            each(1, Y + 1, column)

        far_first(block)

    def shx_whole(g, dev):
        at = hs.at[:, pl.ds(0, SH - SF), rows(g, C // G, C // G)]
        return rdma(at, at, shx_send.at[dev], shx_recv.at[g], {"gr": dev})

    def shared_arrive():
        each(1, G, lambda j: shx_whole(gr_peer(j), gr_peer(j)).wait_recv())

    def ps_copy(t, s):
        return rdma(psh, pshin.at[s], ps_send.at[t], ps_recv.at[s], {"tp": t})

    def shared_first(m):
        part = lax.dot_general(
            xs[rows(si, T, T), 0:C],
            hs[m],
            (((1,), (1,)), ((), ())),
            preferred_element_type=jnp.float32,
        )
        psh[:, m * SH : (m + 1) * SH] = part.astype(jnp.bfloat16)

    def act_arrive():
        for q in range(1, TP):
            for j in range(G):
                a_copy(j, tp_peer(q), tp_peer(q)).wait_recv()

    scope = jax.named_scope

    def peers(order, fn):
        for dist in (int(v) for v in order):
            if dist == 0:
                each(1, Y, lambda k: fn(zi * Y + lax.rem(yi + k, Y)))
            elif dist < Z:

                def row(z):
                    each(0, Y, lambda k: fn(z * Y + lax.rem(yi + k, Y)))

                pl.when(zi + dist < Z)(lambda dist=dist: row(zi + dist))
                pl.when(zi >= dist)(lambda dist=dist: row(zi - dist))

    def weight_out(q, order):
        peers(order, lambda d: w_copy(q, d, si).start())

    def weight_on(q, order):
        def one(s):
            w_copy(q, s, s).wait_recv()
            each(1, G, lambda j: x_copy(q, s, gi, gr_peer(j)).start())

        peers(order, one)

    def settle(kind):
        if kind == "T":
            block_sent(tok_block)
        elif kind == "S":
            sh_sent(sh_block)
        elif kind == "s":
            each(1, G, lambda j: shx_whole(gi, gr_peer(j)).wait_send())
        elif kind == "R":
            for p in range(pieces):
                return_sent(p)
        elif kind == "P":
            for q in range(1, TP):
                t = tp_peer(q)
                for j in range(G):
                    if slots > 1 or j == G - 1:
                        p_copy(j, t, ti, 0).wait_send()
                    a_copy(j, t, ti).wait_send()
        elif kind == "p":
            for q in range(1, TP):
                ps_copy(tp_peer(q), ti).wait_send()
        else:
            q = int(kind)
            m, c, width = parts[q]
            away = wb.at[m, pl.ds(0, S - 1), :, pl.ds(c, width)]
            rdma(away, away, w_send.at[q], w_recv.at[q, si], {"fs": fs_peer(1)}).wait_send()
            each(1, G, lambda j: x_whole(q, gi, gr_peer(j)).wait_send())

    def run(name):
        op, num = name[0], name[1:]
        with scope(name.replace(":", "_")):
            if op == "T":
                spread(tok_block, si, True, True, start)
            elif op == "B":
                pl.semaphore_wait(barrier, S + G + TP - 3)
            elif op == "C":
                m = int(num)
                inputs[1 + m].wait()
                fold(m)
            elif op == "c":
                for m in range(3):
                    inputs[4 + m].wait()
                    fold_shared(m)
            elif op == "X":
                send_own(int(num))
            elif op == "W":
                weight_out(int(num[0]), num[1:])
            elif op == "R":
                relay(tok_block, int(num))
            elif op == "F":
                weight_on(int(num[0]), num[1:])
            elif op == "O":
                others_arrive(tok_block, int(num))
            elif op == "S":
                sh_own(sh_block, start)
            elif op == "s":
                sh_relay(sh_block, int(num), start)
            elif op == "M":
                j = int(num)
                if slots == 1 and j > 0:
                    for q in range(1, TP):
                        p_copy(j - 1, tp_peer(q), ti, 0).wait_send()
                first_matmuls(j)
            elif op == "V":
                activations(int(num))
            elif op == "A":
                for j in range(1, G):
                    x_arrive(int(num), gr_peer(j))
            elif op == "a":
                act_arrive()
            elif op == "D":
                down(int(num))
            elif op == "G":
                gather_far(*(int(v) for v in num.split(":")))
            elif op == "H":
                shared_arrive()
                for m in range(2):
                    shared_first(m)
                for q in range(1, TP):
                    ps_copy(tp_peer(q), ti).start()
            elif op == "P":
                pre = psh[...].astype(jnp.float32)
                for q in range(1, TP):
                    t = tp_peer(q)
                    ps_copy(t, t).wait_recv()
                    pre = pre + pshin[t].astype(jnp.float32)
                shared_act = (silu(pre[:, :SH]) * pre[:, SH:]).astype(jnp.bfloat16)
                rest.append(jnp.dot(shared_act, hs[2], preferred_element_type=jnp.float32))
            elif op == "E":
                for p in range(pieces):
                    gather_near(p)
                total = rest[0] + oz[rows(si, T, T), :].astype(jnp.float32)
                mixed[...] = total.astype(jnp.bfloat16)
            elif op == "w":
                for kind in num:
                    settle(kind)
            else:
                raise ValueError(name)

    rest = []
    with scope("prologue"):
        route_codes()
        inputs[0].wait()
        normalize()
    for name in SCHEDULE:
        run(name)


def emit_kernel(mixed, n0, n1, n2, hs, *refs):
    sem = refs[-1]
    sources = [mixed, n0, n1, n2, hs.at[0], hs.at[1], hs.at[2]]
    copies = []
    for i, (src, dst) in enumerate(zip(sources, refs[:-1])):
        copies.append(pltpu.make_async_copy(src, dst.at[:, 0] if 0 < i < 4 else dst, sem.at[i]))
    for copy in copies:
        copy.start()
    for copy in copies:
        copy.wait()


def emit(results):
    mixed, whole, shared = results[0], results[1], results[4]
    G, H, C = whole.shape
    shapes = [mixed.shape] + [(G, 1, H, C)] * 3 + [shared.shape[1:]] * 3
    return pl.pallas_call(
        emit_kernel,
        out_shape=[jax.ShapeDtypeStruct(s, jnp.bfloat16) for s in shapes],
        in_specs=[pl.BlockSpec(memory_space=pltpu.VMEM)] * len(results),
        out_specs=[pl.BlockSpec(memory_space=pl.ANY)] * len(shapes),
        scratch_shapes=[pltpu.SemaphoreType.DMA((len(shapes),))],
        compiler_params=pltpu.CompilerParams(vmem_limit_bytes=vmem_bytes // 2),
        name="emit",
    )(*results)


def body(
    Y,
    tokens,
    expert_ids,
    route_weight,
    norm_gain,
    expert_gate,
    expert_up,
    expert_down,
    shared_gate,
    shared_up,
    shared_down,
):
    G, S, TP = lax.axis_size("gr"), lax.axis_size("fs"), lax.axis_size("tp")
    T, C = tokens.shape[0], expert_gate.shape[2]
    F, SF = expert_gate.shape[1], shared_gate.shape[0]
    H, SH = F * S, SF * S
    E, N = G * S, S * T
    NH = N // TP
    lanes = -(-2 * E // 128) * 128
    bf16, f32 = jnp.bfloat16, jnp.float32
    halves = 1 if C % 256 == 0 and C >= 1024 else 1
    modes = "A" if C % 512 == 0 and C >= 1024 else "A"
    P = len(modes)
    columns = Y if "B" in modes else 1
    Q = 2 + halves

    out_bytes = 2 * C * (T + 3 * G * H + 3 * SH)
    limit = vmem_bytes - 5 * out_bytes // 4
    fixed = 2 * (N * (3 * C + lanes + G * H) + T * (columns * (S // Y + 1) * C + 2 * SH * (TP + 1)))
    fixed += 6 * 3 * S * F * C + 4 * 3 * SF * C + 2 * T * tokens.shape[1] + 2 * N * G * 2 * H
    slots = G if fixed + 2 * N * G * 2 * H < limit - (1 << 21) else 1
    dims = (G, S, TP, T, C, H, F, SF, slots, Y, halves, modes)
    vmem, hbm = pl.BlockSpec(memory_space=pltpu.VMEM), pl.BlockSpec(memory_space=pl.ANY)
    dma = pltpu.SemaphoreType.DMA
    results = pl.pallas_call(
        functools.partial(handover, dims),
        out_shape=[pltpu.VMEM((T, C), bf16)]
        + [pltpu.VMEM((G, H, C), bf16)] * 3
        + [pltpu.VMEM((3, SH, C), bf16)],
        in_specs=[hbm, vmem, vmem, vmem] + [hbm] * 6,
        out_specs=[vmem] * 5,
        scratch_shapes=[
            pltpu.VMEM(tokens.shape, bf16),
            pltpu.VMEM((3, S, F, C), f32),
            pltpu.VMEM((3, SF, C), f32),
            pltpu.VMEM((3, S, F, C), bf16),
            pltpu.VMEM((N, C + lanes), bf16),
            pltpu.VMEM((slots, TP, NH, 2 * H), bf16),
            pltpu.VMEM((G, max(TP - 1, 1), NH, 2 * H), bf16),
            pltpu.VMEM((G, N, H), bf16),
            pltpu.VMEM((N, C), bf16),
            pltpu.VMEM((P, S // Y, Y, T, C // P), bf16),
            pltpu.VMEM((P, columns, S // Y + 1, T, C // P), bf16),
            pltpu.VMEM((T, 2 * SH), bf16),
            pltpu.VMEM((TP, T, 2 * SH), bf16),
            dma((7,)),
            dma((S, 2 + Y)),
            dma((S,)),
            dma((Q,)),
            dma((Q, S)),
            dma((Q, G)),
            dma((Q, G)),
            dma((S, 2 + Y)),
            dma((S,)),
            dma((G,)),
            dma((G,)),
            dma((G, TP)),
            dma((G, TP)),
            dma((G, TP)),
            dma((G, TP)),
            dma((P, S // Y, Y)),
            dma((P, S // Y, Y)),
            dma((P, columns, S // Y)),
            dma((P, columns, S // Y + 1)),
            dma((TP,)),
            dma((TP,)),
        ],
        compiler_params=pltpu.CompilerParams(
            collective_id=0, has_side_effects=True, vmem_limit_bytes=limit
        ),
        name="handover",
    )(
        tokens,
        expert_ids.T,
        route_weight.T,
        norm_gain[None],
        expert_gate,
        expert_up,
        expert_down,
        shared_gate,
        shared_up,
        shared_down,
    )
    return emit(results)


def line_length(mesh):
    places = [d.coords for d in mesh.devices[0, :, 0]]
    axis = [i for i in range(3) if places[0][i] != places[1][i]][0]
    count = 0
    for place in places:
        if any(place[i] != places[0][i] for i in range(3) if i != axis):
            break
        count += 1
    return count if len(places) % count == 0 else len(places)


def solution(mesh):
    placed = (
        P(("gr", "fs"), None),
        P(("gr", "fs"), None),
        P(("gr", "fs"), None),
        P("tp"),
        P("gr", "fs", "tp"),
        P("gr", "fs", "tp"),
        P("gr", "fs", "tp"),
        P("fs", "tp"),
        P("fs", "tp"),
        P("fs", "tp"),
    )
    return jax.shard_map(
        functools.partial(body, line_length(mesh)),
        mesh=mesh,
        in_specs=placed,
        out_specs=(
            P(("gr", "fs"), "tp"),
            P(None, "fs", None, "tp"),
            P(None, "fs", None, "tp"),
            P(None, "fs", None, "tp"),
            P(None, "tp"),
            P(None, "tp"),
            P(None, "tp"),
        ),
        check_vma=False,
    )
```

```python
import functools

import jax
import jax.numpy as jnp
from jax import lax
from jax.experimental import pallas as pl
from jax.experimental.pallas import tpu as pltpu
from jax.sharding import PartitionSpec as P

SCHEDULE = (
    "B", "T", "C0", "X0", "W001", "C1", "C2", "c", "X1", "X2", "W10", "W20", "R1", "W023", "F00",
    "F01", "F10", "F20", "R2", "W11", "F02", "F03", "R3", "W123", "F11", "W21", "F12", "W22", "F13",
    "W23", "O0", "O1", "O2", "O3", "M0", "F21", "S", "V0", "F22", "F23", "A0", "A1", "M1", "V1",
    "s0", "A2", "a", "D0", "s1", "G0:3", "s2", "wT01", "G0:2", "s3", "w2Ps", "G0:1", "H", "P", "wS",
    "G0:0", "E", "wRp",
)
route_scale = 2.5
norm_eps = 1e-06
vmem_bytes = 67043328


def fold_gain(weight, gain):
    return (weight * gain).astype(jnp.bfloat16)


def silu(v):
    return v / (1.0 + jnp.exp(-v))


def handover(
    dims,
    tok,
    ids,
    scores,
    gain,
    w0,
    w1,
    w2,
    s0,
    s1,
    s2,
    mixed,
    n0,
    n1,
    n2,
    hs,
    tokv,
    wf,
    sf,
    wb,
    xs,
    pout,
    pin,
    act,
    oz,
    rety,
    ret,
    psh,
    pshin,
    in_sem,
    tok_send,
    tok_recv,
    w_send,
    w_recv,
    x_send,
    x_recv,
    sh_send,
    sh_recv,
    shx_send,
    shx_recv,
    p_send,
    p_recv,
    a_send,
    a_recv,
    ry_send,
    ry_recv,
    r_send,
    r_recv,
    ps_send,
    ps_recv,
):
    G, S, TP, T, C, H, F, SF, slots, Y, halves, modes = dims
    Z = S // Y
    E = G * S
    SH = SF * S
    NB = S // TP
    NH = NB * T
    gi, si, ti = lax.axis_index("gr"), lax.axis_index("fs"), lax.axis_index("tp")
    zi, yi = si // Y, lax.rem(si, Y)
    w, new, sh = (w0, w1, w2), (n0, n1, n2), (s0, s1, s2)
    HW, pieces = C // halves, len(modes)
    CW = C // pieces
    parts = [(0, 0, C), (1, 0, C)] + [(2, h * HW, HW) for h in range(halves)]

    def rdma(src, dst, ssem, rsem, dev):
        return pltpu.make_async_remote_copy(
            src_ref=src,
            dst_ref=dst,
            send_sem=ssem,
            recv_sem=rsem,
            device_id=dev,
            device_id_type=pl.DeviceIdType.MESH,
        )

    def rows(start, step, size):
        return pl.ds(pl.multiple_of(start * step, step), size)

    def each(lo, hi, fn):
        def step(i, c):
            fn(i)
            return c

        lax.fori_loop(lo, hi, step, 0)

    def fs_peer(k):
        return lax.rem(si + k, S)

    def fs_from(k):
        return lax.rem(si + S - k, S)

    def gr_peer(k):
        return lax.rem(gi + k, G)

    def tp_peer(k):
        return lax.rem(ti + k, TP)

    barrier = pltpu.get_barrier_semaphore()

    def greet(axis, peer, n):
        each(
            1,
            n,
            lambda k: pl.semaphore_signal(
                barrier,
                inc=1,
                device_id={axis: peer(k)},
                device_id_type=pl.DeviceIdType.MESH,
            ),
        )

    greet("fs", fs_peer, S)
    greet("gr", gr_peer, G)
    greet("tp", tp_peer, TP)
    inputs = [
        pltpu.make_async_copy(tok, tokv, in_sem.at[0]),
        *(pltpu.make_async_copy(w[m], wf.at[m], in_sem.at[1 + m]) for m in range(3)),
        *(pltpu.make_async_copy(sh[m], sf.at[m], in_sem.at[4 + m]) for m in range(3)),
    ]
    for copy in inputs:
        copy.start()

    def route_codes():
        share = scores[...] / jnp.sum(scores[...], axis=0, keepdims=True) * route_scale
        expert = lax.broadcasted_iota(jnp.int32, (E, T), 0)
        dense = jnp.zeros((E, T), jnp.float32)
        for k in range(ids.shape[0]):
            dense = dense + jnp.where(expert == ids[k : k + 1, :], share[k : k + 1, :], 0.0)
        high = dense.astype(jnp.bfloat16).astype(jnp.float32)
        coded = [high, dense - high]
        if C + 2 * E < xs.shape[1]:
            coded.append(jnp.zeros((xs.shape[1] - C - 2 * E, T), jnp.float32))
        coded = jnp.concatenate(coded, axis=0)
        xs[rows(si, T, T), C:] = coded.T.astype(jnp.bfloat16)

    def normalize():
        def chunk(i):
            at = rows(i, 16, 16)
            x = tokv[at, :].astype(jnp.float32)
            scale = lax.rsqrt(jnp.mean(x * x, axis=1, keepdims=True) + norm_eps)
            mine = tokv[at, rows(ti, C, C)].astype(jnp.float32)
            to = pl.ds(pl.multiple_of(si * T + i * 16, 16), 16)
            xs[to, 0:C] = (mine * scale).astype(jnp.bfloat16)

        each(0, T // 16, chunk)

    def fold(m):
        def one(k):
            d = fs_peer(k)
            value = wf[m, d]
            if m < 2:
                value = value * gain[...]
            value = value.astype(jnp.bfloat16)

            def keep():
                new[m][gi, rows(si, F, F), :] = value

            def away():
                wb[m, d] = value

            pl.when(k == 0)(keep)
            pl.when(k > 0)(away)

        each(0, S, one)

    def fold_shared(m):
        value = sf[m]
        if m < 2:
            value = value * gain[...]
        hs[m, rows(si, SF, SF), :] = value.astype(jnp.bfloat16)

    def w_copy(q, d, s):
        m, c, width = parts[q]
        return rdma(
            wb.at[m, d, :, pl.ds(c, width)],
            new[m].at[gi, rows(s, F, F), pl.ds(c, width)],
            w_send.at[q],
            w_recv.at[q, s],
            {"fs": d},
        )

    def spread(block, s, up, down, act_on):
        place, ssem, rsem, after = block
        at = place(s)

        def hop(way, dev):
            act_on(rdma(at, at, ssem.at[s, way], rsem.at[s], {"fs": dev}))

        if up:
            pl.when(zi < Z - 1)(lambda: hop(0, si + Y))
        if down:
            pl.when(zi > 0)(lambda: hop(1, si - Y))

        def across(k):
            y = lax.rem(yi + k, Y)
            hop(2 + y, zi * Y + y)

        each(1, Y, across)

    def sh_place(s, g):
        return hs.at[:, rows(s, SF, SF), rows(g, C // G, C // G)]

    def shx_copy(s, g, dev):
        at = sh_place(s, g)
        return rdma(at, at, shx_send.at[dev], shx_recv.at[g], {"gr": dev})

    def arrive(block, s):
        place, ssem, rsem, after = block
        rdma(place(s), place(s), ssem.at[s, 0], rsem.at[s], {"fs": fs_peer(1)}).wait_recv()
        if after is not None:
            after(s)

    def start(c):
        c.start()

    def sent(c):
        c.wait_send()

    def relay(block, step, act_on=start):
        def from_below():
            s = si - step * Y
            if act_on is start:
                arrive(block, s)
            spread(block, s, True, False, act_on)

        def from_above():
            s = si + step * Y
            if act_on is start:
                arrive(block, s)
            spread(block, s, False, True, act_on)

        pl.when(zi >= step)(from_below)
        pl.when(zi + step < Z)(from_above)

    def others_arrive(block, step):
        def at(z):
            each(1, Y, lambda k: arrive(block, z * Y + lax.rem(yi + k, Y)))

        if step == 0:
            at(zi)
        else:
            pl.when(zi >= step)(lambda: at(zi - step))
            pl.when(zi + step < Z)(lambda: at(zi + step))

    def block_sent(block):
        spread(block, si, True, True, sent)
        for step in range(1, Z):
            relay(block, step, sent)

    sh_block = (
        lambda s: sh_place(s, gi),
        sh_send,
        sh_recv,
        lambda s: each(1, G, lambda j: shx_copy(s, gi, gr_peer(j)).start()),
    )
    tok_block = (lambda s: xs.at[rows(s, T, T)], tok_send, tok_recv, None)

    def sh_hop(block, s, way, dev, act_on):
        place, ssem, rsem, after = block
        act_on(rdma(place(s), place(s), ssem.at[s, way], rsem.at[s], {"fs": dev}))

    def sh_along(block, s, up, down, act_on):
        if up:
            pl.when(zi < Z - 1)(lambda: sh_hop(block, s, 0, si + Y, act_on))
        if down:
            pl.when(zi > 0)(lambda: sh_hop(block, s, 1, si - Y, act_on))

    def sh_own(block, act_on):
        def across(k):
            y = lax.rem(yi + k, Y)
            sh_hop(block, si, 2 + y, zi * Y + y, act_on)

        each(1, Y, across)
        sh_along(block, si, True, True, act_on)

    def sh_relay(block, step, act_on):
        def one(s, up, down):
            if act_on is start:
                arrive(block, s)
            sh_along(block, s, up, down, act_on)

        if step == 0:
            each(1, Y, lambda k: one(zi * Y + lax.rem(yi + k, Y), True, True))
            return

        def row(z, up):
            each(0, Y, lambda k: one(z * Y + lax.rem(yi + k, Y), up, not up))

        pl.when(zi >= step)(lambda: row(zi - step, True))
        pl.when(zi + step < Z)(lambda: row(zi + step, False))

    def sh_sent(block):
        sh_own(block, sent)
        for step in range(Z):
            sh_relay(block, step, sent)

    def x_copy(q, s, g, dev):
        m, c, width = parts[q]
        place = new[m].at[g, rows(s, F, F), pl.ds(c, width)]
        return rdma(place, place, x_send.at[q, dev], x_recv.at[q, g], {"gr": dev})

    def send_own(q):
        each(1, G, lambda j: x_copy(q, si, gi, gr_peer(j)).start())

    def p_copy(j, t, s):
        return rdma(
            pout.at[j if slots > 1 else 0, t], pin.at[j, s], p_send.at[j, t], p_recv.at[j, s], {"tp": t}
        )

    def a_copy(j, t, s):
        place = act.at[j, rows(s, NH, NH)]
        return rdma(place, place, a_send.at[j, t], a_recv.at[j, s], {"tp": t})

    def first_matmuls(j):
        g = gr_peer(j)
        slot = j if slots > 1 else 0
        for q in range(TP):
            t = tp_peer(1 + q)

            def block(b, t=t):
                x = xs[rows(t * NB + b, T, T), 0:C]
                for m in range(2):
                    part = lax.dot_general(
                        x, new[m][g], (((1,), (1,)), ((), ())), preferred_element_type=jnp.float32
                    )
                    pout[slot, t, rows(b, T, T), m * H : (m + 1) * H] = part.astype(jnp.bfloat16)

            each(0, NB, block)
            if q < TP - 1:
                p_copy(j, t, ti).start()

    def activations(j):
        g = gr_peer(j)
        slot = j if slots > 1 else 0
        expert = g * S + si
        for q in range(1, TP):
            t = tp_peer(q)
            p_copy(j, t, t).wait_recv()

        def block(b):
            r = rows(b, T, T)
            pre = pout[slot, ti, r, :].astype(jnp.float32)
            for q in range(1, TP):
                pre = pre + pin[j, tp_peer(q), r, :].astype(jnp.float32)
            at = rows(ti * NB + b, T, T)
            coded = xs[at, C:].astype(jnp.float32)
            lane = lax.broadcasted_iota(jnp.int32, coded.shape, 1)
            share = jnp.sum(
                jnp.where((lane == expert) | (lane == expert + E), coded, 0.0), axis=1, keepdims=True
            )
            value = silu(pre[:, :H]) * pre[:, H:] * share
            act[j, at, :] = value.astype(jnp.bfloat16)

        each(0, NB, block)
        for q in range(1, TP):
            a_copy(j, tp_peer(q), ti).start()

    def p_copy(j, t, s, place):
        return rdma(
            pout.at[j if slots > 1 else 0, t],
            pin.at[j, place],
            p_send.at[j, t],
            p_recv.at[j, s],
            {"tp": t},
        )

    def a_copy(j, t, s):
        place = act.at[j, rows(s, NH, NH)]
        return rdma(place, place, a_send.at[j, t], a_recv.at[j, s], {"tp": t})

    PB = 2 if NB % 2 == 0 else 1

    def first_matmuls(j):
        g = gr_peer(j)
        slot = j if slots > 1 else 0
        for q in range(TP):
            t = tp_peer(1 + q)

            def block(b, t=t):
                x = xs[pl.ds(pl.multiple_of((t * NB + b * PB) * T, T), PB * T), 0:C]
                for m in range(2):
                    part = lax.dot_general(
                        x, new[m][g], (((1,), (1,)), ((), ())), preferred_element_type=jnp.float32
                    )
                    at = pl.ds(pl.multiple_of(b * PB * T, T), PB * T)
                    pout[slot, t, at, m * H : (m + 1) * H] = part.astype(jnp.bfloat16)

            each(0, NB // PB, block)
            if q < TP - 1:
                p_copy(j, t, ti, TP - 2 - q).start()

    def activations(j):
        g = gr_peer(j)
        slot = j if slots > 1 else 0
        expert = g * S + si
        for q in range(1, TP):
            t = tp_peer(q)
            p_copy(j, t, t, q - 1).wait_recv()

        def block(b):
            r = rows(b, T, T)
            pre = pout[slot, ti, r, :].astype(jnp.float32)
            for q in range(1, TP):
                pre = pre + pin[j, q - 1, r, :].astype(jnp.float32)
            at = rows(ti * NB + b, T, T)
            coded = xs[at, C:].astype(jnp.float32)
            lane = lax.broadcasted_iota(jnp.int32, coded.shape, 1)
            share = jnp.sum(
                jnp.where((lane == expert) | (lane == expert + E), coded, 0.0), axis=1, keepdims=True
            )
            value = silu(pre[:, :H]) * pre[:, H:] * share
            act[j, at, :] = value.astype(jnp.bfloat16)

        each(0, NB, block)
        for q in range(1, TP):
            a_copy(j, tp_peer(q), ti).start()

    def x_whole(q, g, dev):
        m, c, width = parts[q]
        place = new[m].at[g, :, pl.ds(c, width)]
        return rdma(place, place, x_send.at[q, dev], x_recv.at[q, g], {"gr": dev})

    def x_arrive(q, g):
        x_whole(q, g, g).wait_recv()

    def piece(p):
        return pl.ds(p * CW, CW)

    def ry_copy(p, z, y, src):
        return rdma(
            oz.at[rows(z * Y + y, T, T), piece(p)],
            rety.at[p, z, src],
            ry_send.at[p, z, y],
            ry_recv.at[p, z, src],
            {"fs": zi * Y + y},
        )

    def r_copy(p, z, y, col, up, dist):
        slot = Z if dist == 1 and not up else z
        return rdma(
            oz.at[rows(z * Y + y, T, T), piece(p)],
            ret.at[p, col, slot],
            r_send.at[p, col, z],
            r_recv.at[p, col, slot],
            {"fs": si + Y if up else si - Y},
        )

    def far_first(fn, only=None):
        for dist in range(Z - 1, -1, -1):
            if only is not None and dist != only:
                continue
            pl.when(zi + dist < Z)(functools.partial(fn, zi + dist, True, dist))
            if dist:
                pl.when(zi >= dist)(functools.partial(fn, zi - dist, False, dist))

    def down(p):
        def block(z, up, dist):
            def column(k):
                y = lax.rem(yi + k, Y)
                at = rows(z * Y + y, T, T)
                total = jnp.zeros((T, CW), jnp.float32)
                for j in range(G):
                    total = total + jnp.dot(
                        act[j, at, :], new[2][gr_peer(j), :, piece(p)], preferred_element_type=jnp.float32
                    )
                oz[at, piece(p)] = total.astype(jnp.bfloat16)
                if modes[p] == "A":
                    pl.when(y != yi)(lambda: ry_copy(p, z, y, yi).start())
                elif dist:
                    ends = zi == 0 if up else zi == Z - 1
                    pl.when(ends)(lambda: r_copy(p, z, y, y, up, dist).start())

            each(1, Y + 1, column)

        far_first(block)

    def chain(p, z, y, col, up, dist, final=False):
        at = rows(z * Y + y, T, T)

        def add_far(slot):
            rdma(
                ret.at[p, col, slot],
                ret.at[p, col, slot],
                r_send.at[p, col, z],
                r_recv.at[p, col, slot],
                {"fs": fs_peer(1)},
            ).wait_recv()
            total = oz[at, piece(p)].astype(jnp.float32) + ret[p, col, slot].astype(jnp.float32)
            oz[at, piece(p)] = total.astype(jnp.bfloat16)

        inner = True
        if dist == 0 or up:
            inner = zi > 0
            pl.when(zi > 0)(lambda: add_far(z))
        if dist == 0:
            pl.when(zi < Z - 1)(lambda: add_far(Z))
        elif not up:
            inner = zi < Z - 1
            pl.when(zi < Z - 1)(lambda: add_far(z))
        if dist:
            if modes[p] == "A":
                r_copy(p, z, y, col, up, dist).start()
            else:
                pl.when(inner)(lambda: r_copy(p, z, y, col, up, dist).start())

    def across_sum(p, z):
        at = rows(z * Y + yi, T, T)
        total = oz[at, piece(p)].astype(jnp.float32)
        for k in range(1, Y):
            y = lax.rem(yi + k, Y)
            ry_copy(p, z, y, y).wait_recv()
            total = total + rety[p, z, y].astype(jnp.float32)
        oz[at, piece(p)] = total.astype(jnp.bfloat16)

    def gather_far(p, only=None):
        def block(z, up, dist):
            if modes[p] == "A":
                across_sum(p, z)
                chain(p, z, yi, 0, up, dist)
                return

            def column(k):
                y = lax.rem(yi + k, Y)
                chain(p, z, y, y, up, dist)
                if dist == 0:
                    pl.when(y != yi)(lambda: ry_copy(p, z, y, yi).start())

            each(1, Y + 1, column)

        far_first(block, only)

    def gather_near(p):
        if modes[p] == "B":
            across_sum(p, zi)

    def return_sent(p):
        def block(z, up, dist):
            def column(k):
                y = lax.rem(yi + k, Y)
                if modes[p] == "A":
                    pl.when(y != yi)(lambda: ry_copy(p, z, y, yi).wait_send())
                    if dist:
                        pl.when(y == yi)(lambda: r_copy(p, z, y, 0, up, dist).wait_send())
                elif dist:
                    r_copy(p, z, y, y, up, dist).wait_send()
                else:
                    pl.when(y != yi)(lambda: ry_copy(p, z, y, yi).wait_send())

            each(1, Y + 1, column)

        far_first(block)

    def shx_whole(g, dev):
        at = hs.at[:, pl.ds(0, SH - SF), rows(g, C // G, C // G)]
        return rdma(at, at, shx_send.at[dev], shx_recv.at[g], {"gr": dev})

    def shared_arrive():
        each(1, G, lambda j: shx_whole(gr_peer(j), gr_peer(j)).wait_recv())

    def ps_copy(t, s):
        return rdma(psh, pshin.at[s], ps_send.at[t], ps_recv.at[s], {"tp": t})

    def shared_first(m):
        part = lax.dot_general(
            xs[rows(si, T, T), 0:C],
            hs[m],
            (((1,), (1,)), ((), ())),
            preferred_element_type=jnp.float32,
        )
        psh[:, m * SH : (m + 1) * SH] = part.astype(jnp.bfloat16)

    def act_arrive():
        for q in range(1, TP):
            for j in range(G):
                a_copy(j, tp_peer(q), tp_peer(q)).wait_recv()

    scope = jax.named_scope

    def peers(order, fn):
        for dist in (int(v) for v in order):
            if dist == 0:
                each(1, Y, lambda k: fn(zi * Y + lax.rem(yi + k, Y)))
            elif dist < Z:

                def row(z):
                    each(0, Y, lambda k: fn(z * Y + lax.rem(yi + k, Y)))

                pl.when(zi + dist < Z)(lambda dist=dist: row(zi + dist))
                pl.when(zi >= dist)(lambda dist=dist: row(zi - dist))

    def weight_out(q, order):
        peers(order, lambda d: w_copy(q, d, si).start())

    def weight_on(q, order):
        def one(s):
            w_copy(q, s, s).wait_recv()
            each(1, G, lambda j: x_copy(q, s, gi, gr_peer(j)).start())

        peers(order, one)

    def settle(kind):
        if kind == "T":
            block_sent(tok_block)
        elif kind == "S":
            sh_sent(sh_block)
        elif kind == "s":
            each(1, G, lambda j: shx_whole(gi, gr_peer(j)).wait_send())
        elif kind == "R":
            for p in range(pieces):
                return_sent(p)
        elif kind == "P":
            for q in range(1, TP):
                t = tp_peer(q)
                for j in range(G):
                    if slots > 1 or j == G - 1:
                        p_copy(j, t, ti, 0).wait_send()
                    a_copy(j, t, ti).wait_send()
        elif kind == "p":
            for q in range(1, TP):
                ps_copy(tp_peer(q), ti).wait_send()
        else:
            q = int(kind)
            m, c, width = parts[q]
            away = wb.at[m, pl.ds(0, S - 1), :, pl.ds(c, width)]
            rdma(away, away, w_send.at[q], w_recv.at[q, si], {"fs": fs_peer(1)}).wait_send()
            each(1, G, lambda j: x_whole(q, gi, gr_peer(j)).wait_send())

    def run(name):
        op, num = name[0], name[1:]
        with scope(name.replace(":", "_")):
            if op == "T":
                spread(tok_block, si, True, True, start)
            elif op == "B":
                pl.semaphore_wait(barrier, S + G + TP - 3)
            elif op == "C":
                m = int(num)
                inputs[1 + m].wait()
                fold(m)
            elif op == "c":
                for m in range(3):
                    inputs[4 + m].wait()
                    fold_shared(m)
            elif op == "X":
                send_own(int(num))
            elif op == "W":
                weight_out(int(num[0]), num[1:])
            elif op == "R":
                relay(tok_block, int(num))
            elif op == "F":
                weight_on(int(num[0]), num[1:])
            elif op == "O":
                others_arrive(tok_block, int(num))
            elif op == "S":
                sh_own(sh_block, start)
            elif op == "s":
                sh_relay(sh_block, int(num), start)
            elif op == "M":
                j = int(num)
                if slots == 1 and j > 0:
                    for q in range(1, TP):
                        p_copy(j - 1, tp_peer(q), ti, 0).wait_send()
                first_matmuls(j)
            elif op == "V":
                activations(int(num))
            elif op == "A":
                for j in range(1, G):
                    x_arrive(int(num), gr_peer(j))
            elif op == "a":
                act_arrive()
            elif op == "D":
                down(int(num))
            elif op == "G":
                gather_far(*(int(v) for v in num.split(":")))
            elif op == "H":
                shared_arrive()
                for m in range(2):
                    shared_first(m)
                for q in range(1, TP):
                    ps_copy(tp_peer(q), ti).start()
            elif op == "P":
                pre = psh[...].astype(jnp.float32)
                for q in range(1, TP):
                    t = tp_peer(q)
                    ps_copy(t, t).wait_recv()
                    pre = pre + pshin[t].astype(jnp.float32)
                shared_act = (silu(pre[:, :SH]) * pre[:, SH:]).astype(jnp.bfloat16)
                rest.append(jnp.dot(shared_act, hs[2], preferred_element_type=jnp.float32))
            elif op == "E":
                for p in range(pieces):
                    gather_near(p)
                total = rest[0] + oz[rows(si, T, T), :].astype(jnp.float32)
                mixed[...] = total.astype(jnp.bfloat16)
            elif op == "w":
                for kind in num:
                    settle(kind)
            else:
                raise ValueError(name)

    rest = []
    with scope("prologue"):
        route_codes()
        inputs[0].wait()
        normalize()
    for name in SCHEDULE:
        run(name)


def emit_kernel(mixed, n0, n1, n2, hs, *refs):
    sem = refs[-1]
    sources = [mixed, n0, n1, n2, hs.at[0], hs.at[1], hs.at[2]]
    copies = []
    for i, (src, dst) in enumerate(zip(sources, refs[:-1])):
        copies.append(pltpu.make_async_copy(src, dst.at[:, 0] if 0 < i < 4 else dst, sem.at[i]))
    for copy in copies:
        copy.start()
    for copy in copies:
        copy.wait()


def emit(results):
    mixed, whole, shared = results[0], results[1], results[4]
    G, H, C = whole.shape
    shapes = [mixed.shape] + [(G, 1, H, C)] * 3 + [shared.shape[1:]] * 3
    return pl.pallas_call(
        emit_kernel,
        out_shape=[jax.ShapeDtypeStruct(s, jnp.bfloat16) for s in shapes],
        in_specs=[pl.BlockSpec(memory_space=pltpu.VMEM)] * len(results),
        out_specs=[pl.BlockSpec(memory_space=pl.ANY)] * len(shapes),
        scratch_shapes=[pltpu.SemaphoreType.DMA((len(shapes),))],
        compiler_params=pltpu.CompilerParams(vmem_limit_bytes=vmem_bytes // 2),
        name="emit",
    )(*results)


def body(
    Y,
    tokens,
    expert_ids,
    route_weight,
    norm_gain,
    expert_gate,
    expert_up,
    expert_down,
    shared_gate,
    shared_up,
    shared_down,
):
    G, S, TP = lax.axis_size("gr"), lax.axis_size("fs"), lax.axis_size("tp")
    T, C = tokens.shape[0], expert_gate.shape[2]
    F, SF = expert_gate.shape[1], shared_gate.shape[0]
    H, SH = F * S, SF * S
    E, N = G * S, S * T
    NH = N // TP
    lanes = -(-2 * E // 128) * 128
    bf16, f32 = jnp.bfloat16, jnp.float32
    halves = 1 if C % 256 == 0 and C >= 1024 else 1
    modes = "A"
    P = len(modes)
    columns = Y if "B" in modes else 1
    Q = 2 + halves

    out_bytes = 2 * C * (T + 3 * G * H + 3 * SH)
    limit = vmem_bytes - 5 * out_bytes // 4
    fixed = 2 * (N * (3 * C + lanes + G * H) + T * (columns * (S // Y + 1) * C + 2 * SH * (TP + 1)))
    fixed += 6 * 3 * S * F * C + 4 * 3 * SF * C + 2 * T * tokens.shape[1] + 2 * N * G * 2 * H
    slots = G if fixed + 2 * N * G * 2 * H < limit - (1 << 21) else 1
    dims = (G, S, TP, T, C, H, F, SF, slots, Y, halves, modes)
    vmem, hbm = pl.BlockSpec(memory_space=pltpu.VMEM), pl.BlockSpec(memory_space=pl.ANY)
    dma = pltpu.SemaphoreType.DMA
    results = pl.pallas_call(
        functools.partial(handover, dims),
        out_shape=[pltpu.VMEM((T, C), bf16)]
        + [pltpu.VMEM((G, H, C), bf16)] * 3
        + [pltpu.VMEM((3, SH, C), bf16)],
        in_specs=[hbm, vmem, vmem, vmem] + [hbm] * 6,
        out_specs=[vmem] * 5,
        scratch_shapes=[
            pltpu.VMEM(tokens.shape, bf16),
            pltpu.VMEM((3, S, F, C), f32),
            pltpu.VMEM((3, SF, C), f32),
            pltpu.VMEM((3, S, F, C), bf16),
            pltpu.VMEM((N, C + lanes), bf16),
            pltpu.VMEM((slots, TP, NH, 2 * H), bf16),
            pltpu.VMEM((G, max(TP - 1, 1), NH, 2 * H), bf16),
            pltpu.VMEM((G, N, H), bf16),
            pltpu.VMEM((N, C), bf16),
            pltpu.VMEM((P, S // Y, Y, T, C // P), bf16),
            pltpu.VMEM((P, columns, S // Y + 1, T, C // P), bf16),
            pltpu.VMEM((T, 2 * SH), bf16),
            pltpu.VMEM((TP, T, 2 * SH), bf16),
            dma((7,)),
            dma((S, 2 + Y)),
            dma((S,)),
            dma((Q,)),
            dma((Q, S)),
            dma((Q, G)),
            dma((Q, G)),
            dma((S, 2 + Y)),
            dma((S,)),
            dma((G,)),
            dma((G,)),
            dma((G, TP)),
            dma((G, TP)),
            dma((G, TP)),
            dma((G, TP)),
            dma((P, S // Y, Y)),
            dma((P, S // Y, Y)),
            dma((P, columns, S // Y)),
            dma((P, columns, S // Y + 1)),
            dma((TP,)),
            dma((TP,)),
        ],
        compiler_params=pltpu.CompilerParams(
            collective_id=0, has_side_effects=True, vmem_limit_bytes=limit
        ),
        name="handover",
    )(
        tokens,
        expert_ids.T,
        route_weight.T,
        norm_gain[None],
        expert_gate,
        expert_up,
        expert_down,
        shared_gate,
        shared_up,
        shared_down,
    )
    return emit(results)


def line_length(mesh):
    places = [d.coords for d in mesh.devices[0, :, 0]]
    axis = [i for i in range(3) if places[0][i] != places[1][i]][0]
    count = 0
    for place in places:
        if any(place[i] != places[0][i] for i in range(3) if i != axis):
            break
        count += 1
    return count if len(places) % count == 0 else len(places)


def solution(mesh):
    placed = (
        P(("gr", "fs"), None),
        P(("gr", "fs"), None),
        P(("gr", "fs"), None),
        P("tp"),
        P("gr", "fs", "tp"),
        P("gr", "fs", "tp"),
        P("gr", "fs", "tp"),
        P("fs", "tp"),
        P("fs", "tp"),
        P("fs", "tp"),
    )
    return jax.shard_map(
        functools.partial(body, line_length(mesh)),
        mesh=mesh,
        in_specs=placed,
        out_specs=(
            P(("gr", "fs"), "tp"),
            P(None, "fs", None, "tp"),
            P(None, "fs", None, "tp"),
            P(None, "fs", None, "tp"),
            P(None, "tp"),
            P(None, "tp"),
            P(None, "tp"),
        ),
        check_vma=False,
    )
```

```python
import functools

import jax
import jax.numpy as jnp
from jax import lax
from jax.experimental import pallas as pl
from jax.experimental.pallas import tpu as pltpu
from jax.sharding import PartitionSpec as P

SCHEDULE = (
    "B", "T", "C0", "X0", "W001", "C1", "C2", "c", "X1", "X2", "W10", "W20", "R1", "W023", "F00",
    "F01", "F10", "F20", "R2", "W11", "F02", "F03", "R3", "W123", "F11", "W21", "F12", "W22", "F13",
    "W23", "O0", "O1", "O2", "O3", "M0", "F21", "S", "V0", "F22", "F23", "A0", "A1", "M1", "V1",
    "s0", "A2", "a", "D0", "s1", "G0:3", "s2", "wT01", "G0:2", "s3", "w2Ps", "G0:1", "H", "P", "wS",
    "G0:0", "E", "wRp",
)
route_scale = 2.5
norm_eps = 1e-06
vmem_bytes = 67043328


def fold_gain(weight, gain):
    return (weight * gain).astype(jnp.bfloat16)


def silu(v):
    return v / (1.0 + jnp.exp(-v))


def handover(
    dims,
    tok,
    ids,
    scores,
    gain,
    w0,
    w1,
    w2,
    s0,
    s1,
    s2,
    mixed,
    n0,
    n1,
    n2,
    hs,
    tokv,
    wf,
    sf,
    wb,
    xs,
    pout,
    pin,
    act,
    oz,
    rety,
    ret,
    psh,
    pshin,
    in_sem,
    tok_send,
    tok_recv,
    w_send,
    w_recv,
    x_send,
    x_recv,
    sh_send,
    sh_recv,
    shx_send,
    shx_recv,
    p_send,
    p_recv,
    a_send,
    a_recv,
    ry_send,
    ry_recv,
    r_send,
    r_recv,
    ps_send,
    ps_recv,
):
    G, S, TP, T, C, H, F, SF, slots, Y, halves, modes = dims
    Z = S // Y
    E = G * S
    SH = SF * S
    NB = S // TP
    NH = NB * T
    gi, si, ti = lax.axis_index("gr"), lax.axis_index("fs"), lax.axis_index("tp")
    zi, yi = si // Y, lax.rem(si, Y)
    w, new, sh = (w0, w1, w2), (n0, n1, n2), (s0, s1, s2)
    HW, pieces = C // halves, len(modes)
    CW = C // pieces
    parts = [(0, 0, C), (1, 0, C)] + [(2, h * HW, HW) for h in range(halves)]

    def rdma(src, dst, ssem, rsem, dev):
        return pltpu.make_async_remote_copy(
            src_ref=src,
            dst_ref=dst,
            send_sem=ssem,
            recv_sem=rsem,
            device_id=dev,
            device_id_type=pl.DeviceIdType.MESH,
        )

    def rows(start, step, size):
        return pl.ds(pl.multiple_of(start * step, step), size)

    def each(lo, hi, fn):
        def step(i, c):
            fn(i)
            return c

        lax.fori_loop(lo, hi, step, 0)

    def fs_peer(k):
        return lax.rem(si + k, S)

    def fs_from(k):
        return lax.rem(si + S - k, S)

    def gr_peer(k):
        return lax.rem(gi + k, G)

    def tp_peer(k):
        return lax.rem(ti + k, TP)

    barrier = pltpu.get_barrier_semaphore()

    def greet(axis, peer, n):
        each(
            1,
            n,
            lambda k: pl.semaphore_signal(
                barrier,
                inc=1,
                device_id={axis: peer(k)},
                device_id_type=pl.DeviceIdType.MESH,
            ),
        )

    greet("fs", fs_peer, S)
    greet("gr", gr_peer, G)
    greet("tp", tp_peer, TP)
    inputs = [
        pltpu.make_async_copy(tok, tokv, in_sem.at[0]),
        *(pltpu.make_async_copy(w[m], wf.at[m], in_sem.at[1 + m]) for m in range(3)),
        *(pltpu.make_async_copy(sh[m], sf.at[m], in_sem.at[4 + m]) for m in range(3)),
    ]
    for copy in inputs:
        copy.start()

    def route_codes():
        share = scores[...] / jnp.sum(scores[...], axis=0, keepdims=True) * route_scale
        expert = lax.broadcasted_iota(jnp.int32, (E, T), 0)
        dense = jnp.zeros((E, T), jnp.float32)
        for k in range(ids.shape[0]):
            dense = dense + jnp.where(expert == ids[k : k + 1, :], share[k : k + 1, :], 0.0)
        high = dense.astype(jnp.bfloat16).astype(jnp.float32)
        coded = [high, dense - high]
        if C + 2 * E < xs.shape[1]:
            coded.append(jnp.zeros((xs.shape[1] - C - 2 * E, T), jnp.float32))
        coded = jnp.concatenate(coded, axis=0)
        xs[rows(si, T, T), C:] = coded.T.astype(jnp.bfloat16)

    def normalize():
        def chunk(i):
            at = rows(i, 16, 16)
            x = tokv[at, :].astype(jnp.float32)
            scale = lax.rsqrt(jnp.mean(x * x, axis=1, keepdims=True) + norm_eps)
            mine = tokv[at, rows(ti, C, C)].astype(jnp.float32)
            to = pl.ds(pl.multiple_of(si * T + i * 16, 16), 16)
            xs[to, 0:C] = (mine * scale).astype(jnp.bfloat16)

        each(0, T // 16, chunk)

    def fold(m):
        def one(k):
            d = fs_peer(k)
            value = wf[m, d]
            if m < 2:
                value = value * gain[...]
            value = value.astype(jnp.bfloat16)

            def keep():
                new[m][gi, rows(si, F, F), :] = value

            def away():
                wb[m, d] = value

            pl.when(k == 0)(keep)
            pl.when(k > 0)(away)

        each(0, S, one)

    def fold_shared(m):
        value = sf[m]
        if m < 2:
            value = value * gain[...]
        hs[m, rows(si, SF, SF), :] = value.astype(jnp.bfloat16)

    def w_copy(q, d, s):
        m, c, width = parts[q]
        return rdma(
            wb.at[m, d, :, pl.ds(c, width)],
            new[m].at[gi, rows(s, F, F), pl.ds(c, width)],
            w_send.at[q],
            w_recv.at[q, s],
            {"fs": d},
        )

    def spread(block, s, up, down, act_on):
        place, ssem, rsem, after = block
        at = place(s)

        def hop(way, dev):
            act_on(rdma(at, at, ssem.at[s, way], rsem.at[s], {"fs": dev}))

        if up:
            pl.when(zi < Z - 1)(lambda: hop(0, si + Y))
        if down:
            pl.when(zi > 0)(lambda: hop(1, si - Y))

        def across(k):
            y = lax.rem(yi + k, Y)
            hop(2 + y, zi * Y + y)

        each(1, Y, across)

    def sh_place(s, g):
        return hs.at[:, rows(s, SF, SF), rows(g, C // G, C // G)]

    def shx_copy(s, g, dev):
        at = sh_place(s, g)
        return rdma(at, at, shx_send.at[dev], shx_recv.at[g], {"gr": dev})

    def arrive(block, s):
        place, ssem, rsem, after = block
        rdma(place(s), place(s), ssem.at[s, 0], rsem.at[s], {"fs": fs_peer(1)}).wait_recv()
        if after is not None:
            after(s)

    def start(c):
        c.start()

    def sent(c):
        c.wait_send()

    def relay(block, step, act_on=start):
        def from_below():
            s = si - step * Y
            if act_on is start:
                arrive(block, s)
            spread(block, s, True, False, act_on)

        def from_above():
            s = si + step * Y
            if act_on is start:
                arrive(block, s)
            spread(block, s, False, True, act_on)

        pl.when(zi >= step)(from_below)
        pl.when(zi + step < Z)(from_above)

    def others_arrive(block, step):
        def at(z):
            each(1, Y, lambda k: arrive(block, z * Y + lax.rem(yi + k, Y)))

        if step == 0:
            at(zi)
        else:
            pl.when(zi >= step)(lambda: at(zi - step))
            pl.when(zi + step < Z)(lambda: at(zi + step))

    def block_sent(block):
        spread(block, si, True, True, sent)
        for step in range(1, Z):
            relay(block, step, sent)

    sh_block = (
        lambda s: sh_place(s, gi),
        sh_send,
        sh_recv,
        lambda s: each(1, G, lambda j: shx_copy(s, gi, gr_peer(j)).start()),
    )
    tok_block = (lambda s: xs.at[rows(s, T, T)], tok_send, tok_recv, None)

    def sh_hop(block, s, way, dev, act_on):
        place, ssem, rsem, after = block
        act_on(rdma(place(s), place(s), ssem.at[s, way], rsem.at[s], {"fs": dev}))

    def sh_along(block, s, up, down, act_on):
        if up:
            pl.when(zi < Z - 1)(lambda: sh_hop(block, s, 0, si + Y, act_on))
        if down:
            pl.when(zi > 0)(lambda: sh_hop(block, s, 1, si - Y, act_on))

    def sh_own(block, act_on):
        def across(k):
            y = lax.rem(yi + k, Y)
            sh_hop(block, si, 2 + y, zi * Y + y, act_on)

        each(1, Y, across)
        sh_along(block, si, True, True, act_on)

    def sh_relay(block, step, act_on):
        def one(s, up, down):
            if act_on is start:
                arrive(block, s)
            sh_along(block, s, up, down, act_on)

        if step == 0:
            each(1, Y, lambda k: one(zi * Y + lax.rem(yi + k, Y), True, True))
            return

        def row(z, up):
            each(0, Y, lambda k: one(z * Y + lax.rem(yi + k, Y), up, not up))

        pl.when(zi >= step)(lambda: row(zi - step, True))
        pl.when(zi + step < Z)(lambda: row(zi + step, False))

    def sh_sent(block):
        sh_own(block, sent)
        for step in range(Z):
            sh_relay(block, step, sent)

    def x_copy(q, s, g, dev):
        m, c, width = parts[q]
        place = new[m].at[g, rows(s, F, F), pl.ds(c, width)]
        return rdma(place, place, x_send.at[q, dev], x_recv.at[q, g], {"gr": dev})

    def send_own(q):
        each(1, G, lambda j: x_copy(q, si, gi, gr_peer(j)).start())

    def p_copy(j, t, s):
        return rdma(
            pout.at[j if slots > 1 else 0, t], pin.at[j, s], p_send.at[j, t], p_recv.at[j, s], {"tp": t}
        )

    def a_copy(j, t, s):
        place = act.at[j, rows(s, NH, NH)]
        return rdma(place, place, a_send.at[j, t], a_recv.at[j, s], {"tp": t})

    def first_matmuls(j):
        g = gr_peer(j)
        slot = j if slots > 1 else 0
        for q in range(TP):
            t = tp_peer(1 + q)

            def block(b, t=t):
                x = xs[rows(t * NB + b, T, T), 0:C]
                for m in range(2):
                    part = lax.dot_general(
                        x, new[m][g], (((1,), (1,)), ((), ())), preferred_element_type=jnp.float32
                    )
                    pout[slot, t, rows(b, T, T), m * H : (m + 1) * H] = part.astype(jnp.bfloat16)

            each(0, NB, block)
            if q < TP - 1:
                p_copy(j, t, ti).start()

    def activations(j):
        g = gr_peer(j)
        slot = j if slots > 1 else 0
        expert = g * S + si
        for q in range(1, TP):
            t = tp_peer(q)
            p_copy(j, t, t).wait_recv()

        def block(b):
            r = rows(b, T, T)
            pre = pout[slot, ti, r, :].astype(jnp.float32)
            for q in range(1, TP):
                pre = pre + pin[j, tp_peer(q), r, :].astype(jnp.float32)
            at = rows(ti * NB + b, T, T)
            coded = xs[at, C:].astype(jnp.float32)
            lane = lax.broadcasted_iota(jnp.int32, coded.shape, 1)
            share = jnp.sum(
                jnp.where((lane == expert) | (lane == expert + E), coded, 0.0), axis=1, keepdims=True
            )
            value = silu(pre[:, :H]) * pre[:, H:] * share
            act[j, at, :] = value.astype(jnp.bfloat16)

        each(0, NB, block)
        for q in range(1, TP):
            a_copy(j, tp_peer(q), ti).start()

    def p_copy(j, t, s, place):
        return rdma(
            pout.at[j if slots > 1 else 0, t],
            pin.at[j, place],
            p_send.at[j, t],
            p_recv.at[j, s],
            {"tp": t},
        )

    def a_copy(j, t, s):
        place = act.at[j, rows(s, NH, NH)]
        return rdma(place, place, a_send.at[j, t], a_recv.at[j, s], {"tp": t})

    PB = 4 if NB % 4 == 0 else 2 if NB % 2 == 0 else 1

    def first_matmuls(j):
        g = gr_peer(j)
        slot = j if slots > 1 else 0
        for q in range(TP):
            t = tp_peer(1 + q)

            def block(b, t=t):
                x = xs[pl.ds(pl.multiple_of((t * NB + b * PB) * T, T), PB * T), 0:C]
                for m in range(2):
                    part = lax.dot_general(
                        x, new[m][g], (((1,), (1,)), ((), ())), preferred_element_type=jnp.float32
                    )
                    at = pl.ds(pl.multiple_of(b * PB * T, T), PB * T)
                    pout[slot, t, at, m * H : (m + 1) * H] = part.astype(jnp.bfloat16)

            each(0, NB // PB, block)
            if q < TP - 1:
                p_copy(j, t, ti, TP - 2 - q).start()

    def activations(j):
        g = gr_peer(j)
        slot = j if slots > 1 else 0
        expert = g * S + si
        for q in range(1, TP):
            t = tp_peer(q)
            p_copy(j, t, t, q - 1).wait_recv()

        def block(b):
            r = rows(b, T, T)
            pre = pout[slot, ti, r, :].astype(jnp.float32)
            for q in range(1, TP):
                pre = pre + pin[j, q - 1, r, :].astype(jnp.float32)
            at = rows(ti * NB + b, T, T)
            coded = xs[at, C:].astype(jnp.float32)
            lane = lax.broadcasted_iota(jnp.int32, coded.shape, 1)
            share = jnp.sum(
                jnp.where((lane == expert) | (lane == expert + E), coded, 0.0), axis=1, keepdims=True
            )
            value = silu(pre[:, :H]) * pre[:, H:] * share
            act[j, at, :] = value.astype(jnp.bfloat16)

        each(0, NB, block)
        for q in range(1, TP):
            a_copy(j, tp_peer(q), ti).start()

    def x_whole(q, g, dev):
        m, c, width = parts[q]
        place = new[m].at[g, :, pl.ds(c, width)]
        return rdma(place, place, x_send.at[q, dev], x_recv.at[q, g], {"gr": dev})

    def x_arrive(q, g):
        x_whole(q, g, g).wait_recv()

    def piece(p):
        return pl.ds(p * CW, CW)

    def ry_copy(p, z, y, src):
        return rdma(
            oz.at[rows(z * Y + y, T, T), piece(p)],
            rety.at[p, z, src],
            ry_send.at[p, z, y],
            ry_recv.at[p, z, src],
            {"fs": zi * Y + y},
        )

    def r_copy(p, z, y, col, up, dist):
        slot = Z if dist == 1 and not up else z
        return rdma(
            oz.at[rows(z * Y + y, T, T), piece(p)],
            ret.at[p, col, slot],
            r_send.at[p, col, z],
            r_recv.at[p, col, slot],
            {"fs": si + Y if up else si - Y},
        )

    def far_first(fn, only=None):
        for dist in range(Z - 1, -1, -1):
            if only is not None and dist != only:
                continue
            pl.when(zi + dist < Z)(functools.partial(fn, zi + dist, True, dist))
            if dist:
                pl.when(zi >= dist)(functools.partial(fn, zi - dist, False, dist))

    def down(p):
        def block(z, up, dist):
            def column(k):
                y = lax.rem(yi + k, Y)
                at = rows(z * Y + y, T, T)
                total = jnp.zeros((T, CW), jnp.float32)
                for j in range(G):
                    total = total + jnp.dot(
                        act[j, at, :], new[2][gr_peer(j), :, piece(p)], preferred_element_type=jnp.float32
                    )
                oz[at, piece(p)] = total.astype(jnp.bfloat16)
                if modes[p] == "A":
                    pl.when(y != yi)(lambda: ry_copy(p, z, y, yi).start())
                elif dist:
                    ends = zi == 0 if up else zi == Z - 1
                    pl.when(ends)(lambda: r_copy(p, z, y, y, up, dist).start())

            each(1, Y + 1, column)

        far_first(block)

    def chain(p, z, y, col, up, dist, final=False):
        at = rows(z * Y + y, T, T)

        def add_far(slot):
            rdma(
                ret.at[p, col, slot],
                ret.at[p, col, slot],
                r_send.at[p, col, z],
                r_recv.at[p, col, slot],
                {"fs": fs_peer(1)},
            ).wait_recv()
            total = oz[at, piece(p)].astype(jnp.float32) + ret[p, col, slot].astype(jnp.float32)
            oz[at, piece(p)] = total.astype(jnp.bfloat16)

        inner = True
        if dist == 0 or up:
            inner = zi > 0
            pl.when(zi > 0)(lambda: add_far(z))
        if dist == 0:
            pl.when(zi < Z - 1)(lambda: add_far(Z))
        elif not up:
            inner = zi < Z - 1
            pl.when(zi < Z - 1)(lambda: add_far(z))
        if dist:
            if modes[p] == "A":
                r_copy(p, z, y, col, up, dist).start()
            else:
                pl.when(inner)(lambda: r_copy(p, z, y, col, up, dist).start())

    def across_sum(p, z):
        at = rows(z * Y + yi, T, T)
        total = oz[at, piece(p)].astype(jnp.float32)
        for k in range(1, Y):
            y = lax.rem(yi + k, Y)
            ry_copy(p, z, y, y).wait_recv()
            total = total + rety[p, z, y].astype(jnp.float32)
        oz[at, piece(p)] = total.astype(jnp.bfloat16)

    def gather_far(p, only=None):
        def block(z, up, dist):
            if modes[p] == "A":
                across_sum(p, z)
                chain(p, z, yi, 0, up, dist)
                return

            def column(k):
                y = lax.rem(yi + k, Y)
                chain(p, z, y, y, up, dist)
                if dist == 0:
                    pl.when(y != yi)(lambda: ry_copy(p, z, y, yi).start())

            each(1, Y + 1, column)

        far_first(block, only)

    def gather_near(p):
        if modes[p] == "B":
            across_sum(p, zi)

    def return_sent(p):
        def block(z, up, dist):
            def column(k):
                y = lax.rem(yi + k, Y)
                if modes[p] == "A":
                    pl.when(y != yi)(lambda: ry_copy(p, z, y, yi).wait_send())
                    if dist:
                        pl.when(y == yi)(lambda: r_copy(p, z, y, 0, up, dist).wait_send())
                elif dist:
                    r_copy(p, z, y, y, up, dist).wait_send()
                else:
                    pl.when(y != yi)(lambda: ry_copy(p, z, y, yi).wait_send())

            each(1, Y + 1, column)

        far_first(block)

    def shx_whole(g, dev):
        at = hs.at[:, pl.ds(0, SH - SF), rows(g, C // G, C // G)]
        return rdma(at, at, shx_send.at[dev], shx_recv.at[g], {"gr": dev})

    def shared_arrive():
        each(1, G, lambda j: shx_whole(gr_peer(j), gr_peer(j)).wait_recv())

    def ps_copy(t, s):
        return rdma(psh, pshin.at[s], ps_send.at[t], ps_recv.at[s], {"tp": t})

    def shared_first(m):
        part = lax.dot_general(
            xs[rows(si, T, T), 0:C],
            hs[m],
            (((1,), (1,)), ((), ())),
            preferred_element_type=jnp.float32,
        )
        psh[:, m * SH : (m + 1) * SH] = part.astype(jnp.bfloat16)

    def act_arrive():
        for q in range(1, TP):
            for j in range(G):
                a_copy(j, tp_peer(q), tp_peer(q)).wait_recv()

    scope = jax.named_scope

    def peers(order, fn):
        for dist in (int(v) for v in order):
            if dist == 0:
                each(1, Y, lambda k: fn(zi * Y + lax.rem(yi + k, Y)))
            elif dist < Z:

                def row(z):
                    each(0, Y, lambda k: fn(z * Y + lax.rem(yi + k, Y)))

                pl.when(zi + dist < Z)(lambda dist=dist: row(zi + dist))
                pl.when(zi >= dist)(lambda dist=dist: row(zi - dist))

    def weight_out(q, order):
        peers(order, lambda d: w_copy(q, d, si).start())

    def weight_on(q, order):
        def one(s):
            w_copy(q, s, s).wait_recv()
            each(1, G, lambda j: x_copy(q, s, gi, gr_peer(j)).start())

        peers(order, one)

    def settle(kind):
        if kind == "T":
            block_sent(tok_block)
        elif kind == "S":
            sh_sent(sh_block)
        elif kind == "s":
            each(1, G, lambda j: shx_whole(gi, gr_peer(j)).wait_send())
        elif kind == "R":
            for p in range(pieces):
                return_sent(p)
        elif kind == "P":
            for q in range(1, TP):
                t = tp_peer(q)
                for j in range(G):
                    if slots > 1 or j == G - 1:
                        p_copy(j, t, ti, 0).wait_send()
                    a_copy(j, t, ti).wait_send()
        elif kind == "p":
            for q in range(1, TP):
                ps_copy(tp_peer(q), ti).wait_send()
        else:
            q = int(kind)
            m, c, width = parts[q]
            away = wb.at[m, pl.ds(0, S - 1), :, pl.ds(c, width)]
            rdma(away, away, w_send.at[q], w_recv.at[q, si], {"fs": fs_peer(1)}).wait_send()
            each(1, G, lambda j: x_whole(q, gi, gr_peer(j)).wait_send())

    def run(name):
        op, num = name[0], name[1:]
        with scope(name.replace(":", "_")):
            if op == "T":
                spread(tok_block, si, True, True, start)
            elif op == "B":
                pl.semaphore_wait(barrier, S + G + TP - 3)
            elif op == "C":
                m = int(num)
                inputs[1 + m].wait()
                fold(m)
            elif op == "c":
                for m in range(3):
                    inputs[4 + m].wait()
                    fold_shared(m)
            elif op == "X":
                send_own(int(num))
            elif op == "W":
                weight_out(int(num[0]), num[1:])
            elif op == "R":
                relay(tok_block, int(num))
            elif op == "F":
                weight_on(int(num[0]), num[1:])
            elif op == "O":
                others_arrive(tok_block, int(num))
            elif op == "S":
                sh_own(sh_block, start)
            elif op == "s":
                sh_relay(sh_block, int(num), start)
            elif op == "M":
                j = int(num)
                if slots == 1 and j > 0:
                    for q in range(1, TP):
                        p_copy(j - 1, tp_peer(q), ti, 0).wait_send()
                first_matmuls(j)
            elif op == "V":
                activations(int(num))
            elif op == "A":
                for j in range(1, G):
                    x_arrive(int(num), gr_peer(j))
            elif op == "a":
                act_arrive()
            elif op == "D":
                down(int(num))
            elif op == "G":
                gather_far(*(int(v) for v in num.split(":")))
            elif op == "H":
                shared_arrive()
                for m in range(2):
                    shared_first(m)
                for q in range(1, TP):
                    ps_copy(tp_peer(q), ti).start()
            elif op == "P":
                pre = psh[...].astype(jnp.float32)
                for q in range(1, TP):
                    t = tp_peer(q)
                    ps_copy(t, t).wait_recv()
                    pre = pre + pshin[t].astype(jnp.float32)
                shared_act = (silu(pre[:, :SH]) * pre[:, SH:]).astype(jnp.bfloat16)
                rest.append(jnp.dot(shared_act, hs[2], preferred_element_type=jnp.float32))
            elif op == "E":
                for p in range(pieces):
                    gather_near(p)
                total = rest[0] + oz[rows(si, T, T), :].astype(jnp.float32)
                mixed[...] = total.astype(jnp.bfloat16)
            elif op == "w":
                for kind in num:
                    settle(kind)
            else:
                raise ValueError(name)

    rest = []
    with scope("prologue"):
        route_codes()
        inputs[0].wait()
        normalize()
    for name in SCHEDULE:
        run(name)


def emit_kernel(mixed, n0, n1, n2, hs, *refs):
    sem = refs[-1]
    sources = [mixed, n0, n1, n2, hs.at[0], hs.at[1], hs.at[2]]
    pairs = []
    for i, (src, dst) in enumerate(zip(sources, refs[:-1])):
        if 0 < i < 4:
            pairs += [(src.at[g], dst.at[g, 0]) for g in range(src.shape[0])]
        else:
            pairs.append((src, dst))
    copies = [pltpu.make_async_copy(src, dst, sem.at[i]) for i, (src, dst) in enumerate(pairs)]
    for copy in copies:
        copy.start()
    for copy in copies:
        copy.wait()


def emit(results):
    mixed, whole, shared = results[0], results[1], results[4]
    G, H, C = whole.shape
    shapes = [mixed.shape] + [(G, 1, H, C)] * 3 + [shared.shape[1:]] * 3
    return pl.pallas_call(
        emit_kernel,
        out_shape=[jax.ShapeDtypeStruct(s, jnp.bfloat16) for s in shapes],
        in_specs=[pl.BlockSpec(memory_space=pltpu.VMEM)] * len(results),
        out_specs=[pl.BlockSpec(memory_space=pl.ANY)] * len(shapes),
        scratch_shapes=[pltpu.SemaphoreType.DMA((len(shapes) + 3 * (G - 1),))],
        compiler_params=pltpu.CompilerParams(vmem_limit_bytes=vmem_bytes // 2),
        name="emit",
    )(*results)


def body(
    Y,
    tokens,
    expert_ids,
    route_weight,
    norm_gain,
    expert_gate,
    expert_up,
    expert_down,
    shared_gate,
    shared_up,
    shared_down,
):
    G, S, TP = lax.axis_size("gr"), lax.axis_size("fs"), lax.axis_size("tp")
    T, C = tokens.shape[0], expert_gate.shape[2]
    F, SF = expert_gate.shape[1], shared_gate.shape[0]
    H, SH = F * S, SF * S
    E, N = G * S, S * T
    NH = N // TP
    lanes = -(-2 * E // 128) * 128
    bf16, f32 = jnp.bfloat16, jnp.float32
    halves = 1 if C % 256 == 0 and C >= 1024 else 1
    modes = "A"
    P = len(modes)
    columns = Y if "B" in modes else 1
    Q = 2 + halves

    out_bytes = 2 * C * (T + 3 * G * H + 3 * SH)
    limit = vmem_bytes - 5 * out_bytes // 4
    fixed = 2 * (N * (3 * C + lanes + G * H) + T * (columns * (S // Y + 1) * C + 2 * SH * (TP + 1)))
    fixed += 6 * 3 * S * F * C + 4 * 3 * SF * C + 2 * T * tokens.shape[1] + 2 * N * G * 2 * H
    slots = G if fixed + 2 * N * G * 2 * H < limit - (1 << 21) else 1
    dims = (G, S, TP, T, C, H, F, SF, slots, Y, halves, modes)
    vmem, hbm = pl.BlockSpec(memory_space=pltpu.VMEM), pl.BlockSpec(memory_space=pl.ANY)
    dma = pltpu.SemaphoreType.DMA
    results = pl.pallas_call(
        functools.partial(handover, dims),
        out_shape=[pltpu.VMEM((T, C), bf16)]
        + [pltpu.VMEM((G, H, C), bf16)] * 3
        + [pltpu.VMEM((3, SH, C), bf16)],
        in_specs=[hbm, vmem, vmem, vmem] + [hbm] * 6,
        out_specs=[vmem] * 5,
        scratch_shapes=[
            pltpu.VMEM(tokens.shape, bf16),
            pltpu.VMEM((3, S, F, C), f32),
            pltpu.VMEM((3, SF, C), f32),
            pltpu.VMEM((3, S, F, C), bf16),
            pltpu.VMEM((N, C + lanes), bf16),
            pltpu.VMEM((slots, TP, NH, 2 * H), bf16),
            pltpu.VMEM((G, max(TP - 1, 1), NH, 2 * H), bf16),
            pltpu.VMEM((G, N, H), bf16),
            pltpu.VMEM((N, C), bf16),
            pltpu.VMEM((P, S // Y, Y, T, C // P), bf16),
            pltpu.VMEM((P, columns, S // Y + 1, T, C // P), bf16),
            pltpu.VMEM((T, 2 * SH), bf16),
            pltpu.VMEM((TP, T, 2 * SH), bf16),
            dma((7,)),
            dma((S, 2 + Y)),
            dma((S,)),
            dma((Q,)),
            dma((Q, S)),
            dma((Q, G)),
            dma((Q, G)),
            dma((S, 2 + Y)),
            dma((S,)),
            dma((G,)),
            dma((G,)),
            dma((G, TP)),
            dma((G, TP)),
            dma((G, TP)),
            dma((G, TP)),
            dma((P, S // Y, Y)),
            dma((P, S // Y, Y)),
            dma((P, columns, S // Y)),
            dma((P, columns, S // Y + 1)),
            dma((TP,)),
            dma((TP,)),
        ],
        compiler_params=pltpu.CompilerParams(
            collective_id=0, has_side_effects=True, vmem_limit_bytes=limit
        ),
        name="handover",
    )(
        tokens,
        expert_ids.T,
        route_weight.T,
        norm_gain[None],
        expert_gate,
        expert_up,
        expert_down,
        shared_gate,
        shared_up,
        shared_down,
    )
    return emit(results)


def line_length(mesh):
    places = [d.coords for d in mesh.devices[0, :, 0]]
    axis = [i for i in range(3) if places[0][i] != places[1][i]][0]
    count = 0
    for place in places:
        if any(place[i] != places[0][i] for i in range(3) if i != axis):
            break
        count += 1
    return count if len(places) % count == 0 else len(places)


def solution(mesh):
    placed = (
        P(("gr", "fs"), None),
        P(("gr", "fs"), None),
        P(("gr", "fs"), None),
        P("tp"),
        P("gr", "fs", "tp"),
        P("gr", "fs", "tp"),
        P("gr", "fs", "tp"),
        P("fs", "tp"),
        P("fs", "tp"),
        P("fs", "tp"),
    )
    return jax.shard_map(
        functools.partial(body, line_length(mesh)),
        mesh=mesh,
        in_specs=placed,
        out_specs=(
            P(("gr", "fs"), "tp"),
            P(None, "fs", None, "tp"),
            P(None, "fs", None, "tp"),
            P(None, "fs", None, "tp"),
            P(None, "tp"),
            P(None, "tp"),
            P(None, "tp"),
        ),
        check_vma=False,
    )
```
